768 devices in a mesh: fs: 192 (over z, y, core), tp: 4 (over x).
Axes of the slice: x: 4, y: 8, z: 12, core: 2. Of those that a mesh axis runs over, the one named last changes fastest.
Arguments:
- inputs: bfloat16 [196608, 3072], P('fs'), may hold values from -6 to 6
- query_cot: bfloat16 [196608, 768], P('fs', 'tp'), may hold values from -0.0134887695 to 0.0134887695
- value_cot: bfloat16 [196608, 1536], P('fs', 'tp'), may hold values from -0.0134887695 to 0.0134887695
- query_factor: bfloat16 [3072, 192], P('fs'), may hold values from -0.109375 to 0.109375
- value_factor: bfloat16 [3072, 192], P('fs'), may hold values from -0.109375 to 0.109375
- query_weight: float32 [3072, 768], P('fs', 'tp'), may hold values from -0.109375 to 0.109375
- value_weight: float32 [3072, 1536], P('fs', 'tp'), may hold values from -0.109375 to 0.109375
- query_first: float32 [192, 768], P('fs', 'tp'), may hold values from -1.6 to 1.6
- query_second: float32 [192, 768], P('fs', 'tp'), may hold values from 0.002 to 0.05
- value_first: float32 [192, 1536], P('fs', 'tp'), may hold values from -1.6 to 1.6
- value_second: float32 [192, 1536], P('fs', 'tp'), may hold values from 0.002 to 0.05
Outputs:
- step_q: float32 [3072, 768], P('fs', 'tp')
- step_v: float32 [3072, 1536], P('fs', 'tp')
- new_q: float32 [3072, 768], P('fs', 'tp')
- new_v: float32 [3072, 1536], P('fs', 'tp')
- first_q: float32 [192, 768], P('fs', 'tp')
- second_q: float32 [192, 768], P('fs', 'tp')
- first_v: float32 [192, 1536], P('fs', 'tp')
- second_v: float32 [192, 1536], P('fs', 'tp')
- copy_q: bfloat16 [3072, 768], P(None, 'tp')
- copy_v: bfloat16 [3072, 1536], P(None, 'tp')
The draws below stay inside these ranges and needn't reach their ends.
All inputs are finite; a program needn't handle non-finite values.
Results may differ from the reference program's by a relative error of at most 0.0041.
Values may be sent and summed in bfloat16 or wider, within the bound.
No kernel may reach another device: no remote copies, remote signals or barrier semaphores. Data moves between devices by JAX's collectives and lax.ppermute only.
A program may use at most 64 MiB of HBM per device.

```python
import math
import jax
import jax.numpy as jnp
from jax import lax

D = 3072
QW = 768
VW = 1536
R = 192
TOKENS = 196608


def draw_query_first(key, part):
    ramp = 1.0 + 3.0 * jnp.arange(R, dtype=jnp.float32)[:, None] / (R - 1)
    noise = jnp.clip(jax.random.normal(key, (R, QW), jnp.float32), -4.0, 4.0)
    return 0.1 * ramp * noise


def draw_value_first(key, part):
    ramp = 1.0 + 3.0 * jnp.arange(R, dtype=jnp.float32)[:, None] / (R - 1)
    noise = jnp.clip(jax.random.normal(key, (R, VW), jnp.float32), -4.0, 4.0)
    return 0.1 * ramp * noise


def steps_of(stream_key, dims, split, least, largest):
    gain = 1.0
    for axis_at, blocks in split:
        heights = jax.random.uniform(jax.random.fold_in(jax.random.fold_in(stream_key, 6), axis_at), (blocks,), jnp.float32, least / len(split), largest / len(split))
        gain = gain * jnp.repeat(jnp.exp(heights), dims[axis_at] // blocks).reshape((-1,) + (1,) * (len(dims) - 1 - axis_at))
    return gain


def centred(own_key, extent, width, bound, shards=(), kind=jnp.bfloat16):
    factor_of = steps_of(own_key, extent, shards, -0.22, 0.18) if shards else 1.0
    array = jax.random.normal(own_key, extent, jnp.float32) * width * factor_of
    return jnp.minimum(jnp.maximum(array, -bound), bound).astype(kind)


def setup_inputs(seed: int = 0) -> dict:
    streams_of = jax.random.split(jax.random.key(seed), 12)
    return {
        "inputs": centred(streams_of[0], (TOKENS, D), 1.0, 6.0, ((0, 192),)),
        "query_cot": centred(streams_of[1], (TOKENS, QW), (TOKENS ** -0.5), 0.0134887695, ((0, 192), (1, 4))),
        "value_cot": centred(streams_of[2], (TOKENS, VW), (TOKENS ** -0.5), 0.0134887695, ((0, 192), (1, 4))),
        "query_factor": centred(streams_of[3], (D, R), D ** -0.5, 0.109375, ((0, 192),)),
        "value_factor": centred(streams_of[4], (D, R), D ** -0.5, 0.109375, ((0, 192),)),
        "query_weight": centred(streams_of[5], (D, QW), D ** -0.5, 0.109375, ((0, 192), (1, 4)), jnp.float32),
        "value_weight": centred(streams_of[6], (D, VW), D ** -0.5, 0.109375, ((0, 192), (1, 4)), jnp.float32),
        "query_first": draw_query_first(jax.random.fold_in(streams_of[11], 71), 0),
        "query_second": jnp.clip(jnp.exp(math.log(0.05) - 3.218876 * jax.random.uniform(streams_of[8], (R, QW), jnp.float32) ** steps_of(streams_of[8], (R, QW), ((0, 192), (1, 4)), -0.2, 0.2)), 0.002, 0.05),
        "value_first": draw_value_first(jax.random.fold_in(streams_of[11], 71), 0),
        "value_second": jnp.clip(jnp.exp(math.log(0.05) - 3.218876 * jax.random.uniform(streams_of[10], (R, VW), jnp.float32) ** steps_of(streams_of[10], (R, VW), ((0, 192), (1, 4)), -0.2, 0.2)), 0.002, 0.05),
    }


first_decay = 0.9
second_decay = 0.99
small_eps = 1e-08
learn_rate = 0.01

def moments(old_first, old_second, gradient):
    first = first_decay * old_first + (1.0 - first_decay) * gradient
    second = second_decay * old_second + (1.0 - second_decay) * gradient * gradient
    unit = first / (jnp.sqrt(second) + small_eps)
    return (first, second, unit)

def reference(inputs, query_cot, value_cot, query_factor, value_factor, query_weight, value_weight, query_first, query_second, value_first, value_second):
    proj_q = jnp.dot(inputs, query_factor, preferred_element_type=jnp.float32).astype(jnp.bfloat16)
    proj_v = jnp.dot(inputs, value_factor, preferred_element_type=jnp.float32).astype(jnp.bfloat16)
    grad_q = jnp.dot(proj_q.T, query_cot, preferred_element_type=jnp.float32)
    grad_v = jnp.dot(proj_v.T, value_cot, preferred_element_type=jnp.float32)
    first_q, second_q, unit_q = moments(query_first, query_second, grad_q)
    first_v, second_v, unit_v = moments(value_first, value_second, grad_v)
    entries = float(unit_q.size + unit_v.size)
    step_scale = lax.rsqrt((jnp.sum(unit_q * unit_q) + jnp.sum(unit_v * unit_v)) / entries + 1e-06)
    bits_q = (step_scale * unit_q).astype(jnp.bfloat16)
    bits_v = (step_scale * unit_v).astype(jnp.bfloat16)
    step_q = jnp.dot(query_factor, bits_q, preferred_element_type=jnp.float32)
    step_v = jnp.dot(value_factor, bits_v, preferred_element_type=jnp.float32)
    new_q = query_weight - learn_rate * step_q
    new_v = value_weight - learn_rate * step_v
    return (step_q, step_v, new_q, new_v, first_q, second_q, first_v, second_v, new_q.astype(jnp.bfloat16), new_v.astype(jnp.bfloat16))
```

```python
import jax
import jax.numpy as jnp
from jax import lax
from jax.sharding import Mesh
from jax.sharding import PartitionSpec as P

FS = ("fs_0", "fs_1", "fs_2")


first_decay = 0.9
second_decay = 0.99
small_eps = 1e-08
learn_rate = 0.01


def sent_to_all(value, axis):
    size = lax.axis_size(axis)
    return lax.all_to_all(
        jnp.broadcast_to(value[None], (size, *value.shape)), axis, 0, 0, tiled=True
    )


def summed_share(value, axis):
    size = lax.axis_size(axis)
    parts = value.reshape(size, -1, *value.shape[1:])
    return lax.all_to_all(parts, axis, 0, 0, tiled=True).sum(axis=0)


def moments(old_first, old_second, gradient):
    first = first_decay * old_first + (1.0 - first_decay) * gradient
    second = second_decay * old_second + (1.0 - second_decay) * gradient * gradient
    unit = first / (jnp.sqrt(second) + small_eps)
    return (first, second, unit)


def pieces_of(value):
    pieces = []
    for _ in range(3):
        piece = lax.reduce_precision(value, 8, 7)
        pieces.append(piece.astype(jnp.bfloat16))
        value = value - piece
    return pieces


def turned_cols(rank, begin, width):
    n0, n1, n2 = (lax.axis_size(a) for a in FS)
    place = begin + lax.broadcasted_iota(jnp.int32, (rank, width), 1)
    core, rest = place // (n0 * n1), place % (n0 * n1)
    natural = (rest // n1) * (n1 * n2) + (rest % n1) * n2 + core
    row = lax.broadcasted_iota(jnp.int32, (rank, width), 0)
    return (row == natural).astype(jnp.bfloat16)


def exact(a, onehot):
    return jnp.dot(a, onehot, preferred_element_type=jnp.float32).astype(jnp.bfloat16)


def on_device(
    inputs,
    query_cot,
    value_cot,
    query_factor,
    value_factor,
    query_weight,
    value_weight,
    query_first,
    query_second,
    value_first,
    value_second,
):
    n0, n1, n2 = (lax.axis_size(a) for a in FS)
    tp = lax.axis_size("tp")
    own, rank = query_factor.shape
    q_cols = query_cot.shape[1]
    v_cols = value_cot.shape[1]
    cols = q_cols + v_cols
    entries = rank * cols * tp
    width = rank // tp
    bf16 = jnp.bfloat16

    turn = turned_cols(rank, 0, rank)
    factors = exact(jnp.concatenate([value_factor, query_factor], axis=0), turn)
    v_factor, q_factor = factors[:own], factors[own:]

    parcel = jnp.concatenate(
        [v_factor, q_factor, value_weight.astype(bf16), query_weight.astype(bf16)], axis=1
    )
    parcels = lax.all_gather(parcel, FS, axis=0, tiled=True)

    mine = turned_cols(rank, lax.axis_index("tp") * width, width)
    share = exact(jnp.concatenate([value_factor, query_factor], axis=0), mine)
    share = jnp.concatenate([share[:own], share[own:]], axis=1)
    near = sent_to_all(share, "fs_0")
    near = sent_to_all(near, "fs_1")
    near = sent_to_all(near, "fs_2")
    share = near.transpose(2, 1, 0, 3, 4).reshape(-1, 2 * width)
    proj = lax.dot_general(
        share, inputs, (((0,), (1,)), ((), ())), preferred_element_type=jnp.float32
    ).astype(bf16)
    proj = lax.all_gather(proj, "tp", axis=0, tiled=True).reshape(tp, 2, width, -1)
    proj_v = proj[:, 0].reshape(rank, -1)
    proj_q = proj[:, 1].reshape(rank, -1)

    term_v = jnp.dot(proj_v, value_cot, preferred_element_type=jnp.float32)
    term_q = jnp.dot(proj_q, query_cot, preferred_element_type=jnp.float32)
    term = jnp.concatenate([term_v, term_q], axis=1)
    term = summed_share(term, "fs_2")
    term = summed_share(term, "fs_0")
    term = summed_share(term, "fs_1")
    first_v, second_v, unit_v = moments(value_first, value_second, term[:, :v_cols])
    first_q, second_q, unit_q = moments(query_first, query_second, term[:, v_cols:])

    squares = jnp.sum(unit_v * unit_v, axis=1, keepdims=True)
    squares += jnp.sum(unit_q * unit_q, axis=1, keepdims=True)
    spare = -(cols + 3) % 128
    row = jnp.concatenate(
        [
            unit_v.astype(bf16),
            unit_q.astype(bf16),
            *pieces_of(squares),
            jnp.zeros((1, spare), bf16),
        ],
        axis=1,
    )
    rows = sent_to_all(row[0], ("fs_1", "tp")).reshape(n1, tp, -1)
    squares = jnp.sum(rows[:, :, cols : cols + 3].astype(jnp.float32), axis=(1, 2))[:, None]
    rows = lax.dynamic_index_in_dim(rows, lax.axis_index("tp"), 1, keepdims=False)
    rows = jnp.concatenate([rows[:, :cols], *pieces_of(squares), rows[:, cols + 3 :]], axis=1)
    rows = sent_to_all(rows, "fs_0").reshape(n0 * n1, -1)
    rows = sent_to_all(rows, "fs_2").reshape(rank, -1)
    total = jnp.sum(rows[:, cols : cols + 3].astype(jnp.float32))
    scale = lax.rsqrt(total / entries + 1e-06)
    rows_v = rows[:, :v_cols]
    rows_q = rows[:, v_cols:cols]

    step_v = scale * jnp.dot(v_factor, rows_v, preferred_element_type=jnp.float32)
    step_q = scale * jnp.dot(q_factor, rows_q, preferred_element_type=jnp.float32)
    new_v = value_weight - learn_rate * step_v
    new_q = query_weight - learn_rate * step_q

    both = parcels[:, : 2 * rank]
    weights = parcels[:, 2 * rank :].astype(jnp.float32)
    pad_v = jnp.concatenate([rows_v, jnp.zeros_like(rows_v)], axis=0)
    pad_q = jnp.concatenate([jnp.zeros_like(rows_q), rows_q], axis=0)
    rate = learn_rate * scale
    all_v = jnp.dot(both, pad_v, preferred_element_type=jnp.float32)
    all_q = jnp.dot(both, pad_q, preferred_element_type=jnp.float32)
    copy_v = (weights[:, :v_cols] - rate * all_v).astype(bf16)
    copy_q = (weights[:, v_cols:] - rate * all_q).astype(bf16)
    return (step_q, step_v, new_q, new_v, first_q, second_q, first_v, second_v, copy_q, copy_v)


def solution(mesh):
    split = Mesh(mesh.devices.reshape(12, 8, 2, mesh.shape["tp"]), ("fs_0", "fs_1", "fs_2", "tp"))
    return jax.shard_map(
        on_device,
        mesh=split,
        in_specs=(
            P(FS, None),
            P(FS, "tp"),
            P(FS, "tp"),
            P(FS, None),
            P(FS, None),
            P(FS, "tp"),
            P(FS, "tp"),
            P(FS, "tp"),
            P(FS, "tp"),
            P(FS, "tp"),
            P(FS, "tp"),
        ),
        out_specs=(
            P(FS, "tp"),
            P(FS, "tp"),
            P(FS, "tp"),
            P(FS, "tp"),
            P(FS, "tp"),
            P(FS, "tp"),
            P(FS, "tp"),
            P(FS, "tp"),
            P(None, "tp"),
            P(None, "tp"),
        ),
        check_vma=False,
    )
```

```python
import math

import jax
import jax.numpy as jnp
from jax import lax
from jax.experimental import pallas as pl
from jax.experimental.pallas import tpu as pltpu
from jax.sharding import Mesh
from jax.sharding import PartitionSpec as P

FS = ("fs_0", "fs_1", "fs_2")


first_decay = 0.9
second_decay = 0.99
small_eps = 1e-08
learn_rate = 0.01


def sent_to_all(value, axis):
    size = lax.axis_size(axis)
    return lax.all_to_all(
        jnp.broadcast_to(value[None], (size, *value.shape)), axis, 0, 0, tiled=True
    )


def summed_share(value, axis):
    size = lax.axis_size(axis)
    parts = value.reshape(size, -1, *value.shape[1:])
    return lax.all_to_all(parts, axis, 0, 0, tiled=True).sum(axis=0)


def shift_of(size):
    shift = int(math.log2(size))
    assert 1 << shift == size
    return shift


def pack_kernel(at, v_factor, q_factor, v_weight, q_weight, parcel, spread, *, sizes, width):
    own, rank = v_factor.shape
    n0, n1, n2 = sizes
    row = lax.broadcasted_iota(jnp.int32, (rank, rank), 0)
    place = (
        (row & (n2 - 1)) * (n0 * n1)
        + (row >> shift_of(n1 * n2)) * n1
        + ((row >> shift_of(n2)) & (n1 - 1))
    )
    col = lax.broadcasted_iota(jnp.int32, (rank, rank), 1)
    turn = (place == col).astype(jnp.float32).astype(jnp.bfloat16)
    mine = (place == col + at[0] * width) & (col < width)
    mine = mine.astype(jnp.float32).astype(jnp.bfloat16)

    def exact(a, onehot):
        return jnp.dot(a, onehot, preferred_element_type=jnp.float32).astype(jnp.bfloat16)

    vf, qf = v_factor[...], q_factor[...]
    parcel[...] = jnp.concatenate(
        [
            exact(vf, turn),
            exact(qf, turn),
            v_weight[...].astype(jnp.bfloat16),
            q_weight[...].astype(jnp.bfloat16),
        ],
        axis=1,
    )
    share = jnp.concatenate([exact(vf, mine)[:, :width], exact(qf, mine)[:, :width]], axis=1)
    spread[...] = jnp.broadcast_to(share[None], spread.shape)


def pieces_of(value):
    high = value.astype(jnp.bfloat16).astype(jnp.float32)
    middle = (value - high).astype(jnp.bfloat16).astype(jnp.float32)
    return high, middle, value - high - middle


def with_pieces(value, block, at):
    lane = lax.broadcasted_iota(jnp.int32, block.shape, 1)
    for k, piece in enumerate(pieces_of(value)):
        block = jnp.where(lane == at + k, piece, block)
    return block


def moments(old_first, old_second, gradient):
    first = first_decay * old_first + (1.0 - first_decay) * gradient
    second = second_decay * old_second + (1.0 - second_decay) * gradient * gradient
    unit = first / (jnp.sqrt(second) + small_eps)
    return (first, second, unit)


def moments_kernel(terms, v_first, v_second, q_first, q_second, *outs):
    first_v, second_v, first_q, second_q, spread = outs
    v_cols = v_first.shape[1]
    gradient = jnp.sum(terms[...], axis=0)
    first_v[...], second_v[...], unit_v = moments(v_first[...], v_second[...], gradient[:, :v_cols])
    first_q[...], second_q[...], unit_q = moments(q_first[...], q_second[...], gradient[:, v_cols:])
    squares = jnp.sum(unit_v * unit_v, axis=1, keepdims=True)
    squares += jnp.sum(unit_q * unit_q, axis=1, keepdims=True)
    cols = gradient.shape[1]
    lines = -(-(cols + 3) // 128)
    row = jnp.concatenate(
        [unit_v, unit_q, jnp.zeros((1, lines * 128 - cols), jnp.float32)], axis=1
    )
    row = with_pieces(squares, row, cols)
    block = jnp.concatenate(
        [row[:, 128 * k : 128 * (k + 1)] for k in range(lines)]
        + [jnp.zeros((spread.shape[1] - lines, 128), jnp.float32)],
        axis=0,
    ).astype(jnp.bfloat16)
    spread[...] = jnp.broadcast_to(block[None], spread.shape)


def regroup_kernel(at, blocks, spread, *, cols):
    n1, tp = blocks.shape[:2]
    lines = spread.shape[2] // 128
    last, begin = cols // 128, cols % 128
    ends = blocks[:, :, last, :].astype(jnp.float32)
    ends = jnp.sum(ends, axis=1)
    lane = lax.broadcasted_iota(jnp.int32, ends.shape, 1)
    squares = jnp.where((lane >= begin) & (lane < begin + 3), ends, 0.0)
    squares = jnp.sum(squares, axis=1, keepdims=True)
    own = blocks[:, at[0], :, :].astype(jnp.float32)
    parts = [own[:, k, :] for k in range(lines)]
    parts[last] = with_pieces(squares, parts[last], begin)
    rows = jnp.concatenate(parts, axis=1).astype(jnp.bfloat16)
    spread[...] = jnp.broadcast_to(rows[None], spread.shape)


def update_kernel(
    rows, own, v_weight, q_weight, parcels, step_v, step_q, new_v, new_q, copy_v, copy_q, units,
    *, rank, v_cols, q_cols, entries
):
    cols = v_cols + q_cols
    tail = rows[:, cols // 128 * 128 :].astype(jnp.float32)
    lane = lax.broadcasted_iota(jnp.int32, tail.shape, 1) + cols // 128 * 128
    total = jnp.sum(jnp.where((lane >= cols) & (lane < cols + 3), tail, 0.0), keepdims=True)
    scale = lax.rsqrt(total / entries + 1e-06)

    @pl.when(pl.program_id(0) == 0)
    def _():
        units[...] = jnp.zeros(units.shape, units.dtype)
        units[:rank, :v_cols] = rows[:, :v_cols]
        units[rank:, v_cols:] = rows[:, v_cols:cols]
        step = scale * jnp.dot(
            own[:, : 2 * rank], units[...], preferred_element_type=jnp.float32
        )
        step_v[...] = step[:, :v_cols]
        step_q[...] = step[:, v_cols:]
        new_v[...] = v_weight[...] - learn_rate * step[:, :v_cols]
        new_q[...] = q_weight[...] - learn_rate * step[:, v_cols:]

    step = jnp.dot(parcels[:, : 2 * rank], units[...], preferred_element_type=jnp.float32)
    new = parcels[:, 2 * rank :].astype(jnp.float32) - (learn_rate * scale) * step
    copy_v[...] = new[:, :v_cols].astype(jnp.bfloat16)
    copy_q[...] = new[:, v_cols:].T.astype(jnp.bfloat16)


def on_device(
    inputs,
    query_cot,
    value_cot,
    query_factor,
    value_factor,
    query_weight,
    value_weight,
    query_first,
    query_second,
    value_first,
    value_second,
):
    sizes = tuple(lax.axis_size(a) for a in FS)
    n0, n1, n2 = sizes
    tp = lax.axis_size("tp")
    own, rank = query_factor.shape
    q_cols = query_cot.shape[1]
    v_cols = value_cot.shape[1]
    cols = q_cols + v_cols
    width = rank // tp
    whole = rank * own
    bf16, f32 = jnp.bfloat16, jnp.float32
    shape = jax.ShapeDtypeStruct
    vmem = pl.BlockSpec(memory_space=pltpu.VMEM)
    smem = pl.BlockSpec(memory_space=pltpu.SMEM)
    at = lax.axis_index("tp").astype(jnp.int32).reshape(1)

    parcel, spread = pl.pallas_call(
        lambda *refs: pack_kernel(*refs, sizes=sizes, width=width),
        in_specs=[smem] + [vmem] * 4,
        out_specs=[vmem] * 2,
        out_shape=[shape((own, 2 * rank + cols), bf16), shape((n0, own, 2 * width), bf16)],
        name="pack",
    )(at, value_factor, query_factor, value_weight, query_weight)
    parcels = lax.all_gather(parcel, FS, axis=0, tiled=True)

    near = lax.all_to_all(spread, "fs_0", 0, 0, tiled=True)
    near = sent_to_all(near, "fs_1")
    near = sent_to_all(near, "fs_2")
    share = near.transpose(2, 1, 0, 3, 4).reshape(-1, 2 * width)
    proj = lax.dot_general(
        share, inputs, (((0,), (1,)), ((), ())), preferred_element_type=f32
    ).astype(bf16)
    proj = lax.all_gather(proj, "tp", axis=0, tiled=True).reshape(tp, 2, width, -1)
    proj_v = proj[:, 0].reshape(rank, -1)
    proj_q = proj[:, 1].reshape(rank, -1)

    term_v = jnp.dot(proj_v, value_cot, preferred_element_type=f32)
    term_q = jnp.dot(proj_q, query_cot, preferred_element_type=f32)
    term = jnp.concatenate([term_v, term_q], axis=1)
    term = summed_share(term, "fs_2")
    term = summed_share(term, "fs_0")
    term = lax.all_to_all(term.reshape(n1, 1, cols), "fs_1", 0, 0, tiled=True)
    first_v, second_v, first_q, second_q, spread = pl.pallas_call(
        moments_kernel,
        in_specs=[vmem] * 5,
        out_specs=[vmem] * 5,
        out_shape=[shape((1, v_cols), f32)] * 2
        + [shape((1, q_cols), f32)] * 2
        + [shape((n1 * tp, 8, 128), bf16)],
        name="moments",
    )(term, value_first, value_second, query_first, query_second)

    blocks = lax.all_to_all(spread, ("fs_1", "tp"), 0, 0, tiled=True)
    lines = -(-(cols + 3) // 128)
    spread = pl.pallas_call(
        lambda *refs: regroup_kernel(*refs, cols=cols),
        in_specs=[smem, vmem],
        out_specs=vmem,
        out_shape=shape((n0, n1, lines * 128), bf16),
        name="regroup",
    )(at, blocks.reshape(n1, tp, 8, 128))
    rows = lax.all_to_all(spread, "fs_0", 0, 0, tiled=True).reshape(n0 * n1, -1)
    rows = sent_to_all(rows, "fs_2").reshape(rank, -1)

    steps = 8
    block = whole // steps
    fixed = lambda *s: pl.BlockSpec(s, lambda i: (0, 0))
    step_v, step_q, new_v, new_q, copy_v, copy_q = pl.pallas_call(
        lambda *refs: update_kernel(
            *refs, rank=rank, v_cols=v_cols, q_cols=q_cols, entries=rank * cols * tp
        ),
        grid=(steps,),
        in_specs=[
            fixed(rank, lines * 128),
            fixed(own, 2 * rank + cols),
            fixed(own, v_cols),
            fixed(own, q_cols),
            pl.BlockSpec((block, 2 * rank + cols), lambda i: (i, 0)),
        ],
        out_specs=[
            fixed(own, v_cols),
            fixed(own, q_cols),
            fixed(own, v_cols),
            fixed(own, q_cols),
            pl.BlockSpec((block, v_cols), lambda i: (i, 0)),
            pl.BlockSpec((q_cols, block), lambda i: (0, i)),
        ],
        out_shape=[
            shape((own, v_cols), f32),
            shape((own, q_cols), f32),
            shape((own, v_cols), f32),
            shape((own, q_cols), f32),
            shape((whole, v_cols), bf16),
            shape((q_cols, whole), bf16),
        ],
        scratch_shapes=[pltpu.VMEM((2 * rank, cols), bf16)],
        name="update",
    )(rows, parcel, value_weight, query_weight, parcels)
    return (step_q, step_v, new_q, new_v, first_q, second_q, first_v, second_v, copy_q.T, copy_v)


def solution(mesh):
    split = Mesh(mesh.devices.reshape(12, 8, 2, mesh.shape["tp"]), ("fs_0", "fs_1", "fs_2", "tp"))
    return jax.shard_map(
        on_device,
        mesh=split,
        in_specs=(
            P(FS, None),
            P(FS, "tp"),
            P(FS, "tp"),
            P(FS, None),
            P(FS, None),
            P(FS, "tp"),
            P(FS, "tp"),
            P(FS, "tp"),
            P(FS, "tp"),
            P(FS, "tp"),
            P(FS, "tp"),
        ),
        out_specs=(
            P(FS, "tp"),
            P(FS, "tp"),
            P(FS, "tp"),
            P(FS, "tp"),
            P(FS, "tp"),
            P(FS, "tp"),
            P(FS, "tp"),
            P(FS, "tp"),
            P(None, "tp"),
            P(None, "tp"),
        ),
        check_vma=False,
    )
```

```python
import math

import jax
import jax.numpy as jnp
from jax import lax
from jax.experimental import pallas as pl
from jax.experimental.pallas import tpu as pltpu
from jax.sharding import Mesh
from jax.sharding import PartitionSpec as P

FS = ("fs_0", "fs_1", "fs_2")


first_decay = 0.9
second_decay = 0.99
small_eps = 1e-08
learn_rate = 0.01


def sent_to_all(value, axis):
    size = lax.axis_size(axis)
    return lax.all_to_all(
        jnp.broadcast_to(value[None], (size, *value.shape)), axis, 0, 0, tiled=True
    )


def shift_of(size):
    shift = int(math.log2(size))
    assert 1 << shift == size
    return shift


def pack_kernel(at, v_factor, q_factor, v_weight, q_weight, parcel, spread, *, sizes, width):
    own, rank = v_factor.shape
    n0, n1, n2 = sizes
    row = lax.broadcasted_iota(jnp.int32, (rank, rank), 0)
    far = row >> shift_of(n1 * n2)
    place = (row & (n2 - 1)) * (n0 * n1) + far * n1 + ((row >> shift_of(n2)) & (n1 - 1))
    col = lax.broadcasted_iota(jnp.int32, (rank, rank), 1)
    turn = (place == col).astype(jnp.float32).astype(jnp.bfloat16)
    place = (row & (n1 * n2 - 1)) * n0 + far
    mine = (place == col + at[0] * width) & (col < width)
    mine = mine.astype(jnp.float32).astype(jnp.bfloat16)

    def exact(a, onehot):
        return jnp.dot(a, onehot, preferred_element_type=jnp.float32).astype(jnp.bfloat16)

    vf, qf = v_factor[...], q_factor[...]
    parcel[...] = jnp.concatenate(
        [
            exact(vf, turn),
            exact(qf, turn),
            v_weight[...].astype(jnp.bfloat16),
            q_weight[...].astype(jnp.bfloat16),
        ],
        axis=1,
    )
    share = jnp.concatenate([exact(vf, mine)[:, :width], exact(qf, mine)[:, :width]], axis=1)
    spread[...] = jnp.broadcast_to(share[None], spread.shape)


def terms_kernel(proj, v_cot, q_cot, blocks, term_v, term_q, wide, *, n0, width):
    rank, v_cols = term_v.shape
    tp = rank // width
    parts = [proj[2 * width * t : 2 * width * (t + 1), :] for t in range(tp)]
    proj_v = jnp.concatenate([p[:width] for p in parts], axis=0)
    proj_q = jnp.concatenate([p[width:] for p in parts], axis=0)
    term_v[...] = jnp.dot(proj_v, v_cot[...], preferred_element_type=jnp.float32)
    term_q[...] = lax.dot_general(
        proj_q, q_cot[...], (((1,), (1,)), ((), ())), preferred_element_type=jnp.float32
    )
    chunks, half = v_cols // 128, n0 // 2
    wide[...] = jnp.zeros(wide.shape, jnp.float32)
    for b in range(rank // n0):
        for k in range(chunks):
            wide[b, n0 * k : n0 * (k + 1), :] = term_v[
                n0 * b : n0 * (b + 1), 128 * k : 128 * (k + 1)
            ]
        wide[b, n0 * chunks : n0 * (chunks + 1), :] = term_q[n0 * b : n0 * (b + 1), :128]
        rest = jnp.concatenate(
            [term_q[n0 * b : n0 * b + half, 128:], term_q[n0 * b + half : n0 * (b + 1), 128:]],
            axis=1,
        )
        wide[b, n0 * (chunks + 1) : n0 * (chunks + 1) + half, :] = rest
    blocks[...] = wide[...].astype(jnp.bfloat16)


def fold_kernel(blocks, rows, wide, *, n0, chunks):
    wide[...] = jnp.sum(blocks[...].astype(jnp.float32), axis=0)
    half = n0 // 2
    rows[...] = jnp.zeros(rows.shape, jnp.float32)
    for r in range(n0):
        for k in range(chunks + 1):
            rows[r, k : k + 1, :] = wide[n0 * k + r : n0 * k + r + 1, :]
        line = n0 * (chunks + 1) + r % half
        rest = wide[line : line + 1, :]
        if r >= half:
            rest = jnp.concatenate([rest[:, 64:], rest[:, :64]], axis=1)
        rows[r, chunks + 1 : chunks + 2, :] = rest


def pieces_of(value):
    high = value.astype(jnp.bfloat16).astype(jnp.float32)
    middle = (value - high).astype(jnp.bfloat16).astype(jnp.float32)
    return high, middle, value - high - middle


def with_pieces(value, block, at):
    lane = lax.broadcasted_iota(jnp.int32, block.shape, 1)
    for k, piece in enumerate(pieces_of(value)):
        block = jnp.where(lane == at + k, piece, block)
    return block


def moments(old_first, old_second, gradient):
    first = first_decay * old_first + (1.0 - first_decay) * gradient
    second = second_decay * old_second + (1.0 - second_decay) * gradient * gradient
    unit = first / (jnp.sqrt(second) + small_eps)
    return (first, second, unit)


def moments_kernel(terms, v_first, v_second, q_first, q_second, *outs):
    first_v, second_v, first_q, second_q, spread = outs
    v_cols, q_cols = v_first.shape[1], q_first.shape[1]
    gradient = jnp.sum(terms[...], axis=0)
    gradient = jnp.concatenate(
        [gradient[k : k + 1] for k in range(v_cols // 128 + 1)]
        + [gradient[v_cols // 128 + 1 : v_cols // 128 + 2, : q_cols - 128]],
        axis=1,
    )
    first_v[...], second_v[...], unit_v = moments(v_first[...], v_second[...], gradient[:, :v_cols])
    first_q[...], second_q[...], unit_q = moments(q_first[...], q_second[...], gradient[:, v_cols:])
    squares = jnp.sum(unit_v * unit_v, axis=1, keepdims=True)
    squares += jnp.sum(unit_q * unit_q, axis=1, keepdims=True)
    cols = gradient.shape[1]
    lines = -(-(cols + 3) // 128)
    row = jnp.concatenate(
        [unit_v, unit_q, jnp.zeros((1, lines * 128 - cols), jnp.float32)], axis=1
    )
    row = with_pieces(squares, row, cols)
    block = jnp.concatenate(
        [row[:, 128 * k : 128 * (k + 1)] for k in range(lines)]
        + [jnp.zeros((spread.shape[1] - lines, 128), jnp.float32)],
        axis=0,
    ).astype(jnp.bfloat16)
    spread[...] = jnp.broadcast_to(block[None], spread.shape)


def regroup_kernel(at, blocks, spread, *, cols):
    n1, tp = blocks.shape[:2]
    lines = spread.shape[2] // 128
    last, begin = cols // 128, cols % 128
    ends = blocks[:, :, last, :].astype(jnp.float32)
    ends = jnp.sum(ends, axis=1)
    lane = lax.broadcasted_iota(jnp.int32, ends.shape, 1)
    squares = jnp.where((lane >= begin) & (lane < begin + 3), ends, 0.0)
    squares = jnp.sum(squares, axis=1, keepdims=True)
    own = blocks[:, at[0], :, :].astype(jnp.float32)
    parts = [own[:, k, :] for k in range(lines)]
    parts[last] = with_pieces(squares, parts[last], begin)
    rows = jnp.concatenate(parts, axis=1).astype(jnp.bfloat16)
    spread[...] = jnp.broadcast_to(rows[None], spread.shape)


def update_kernel(
    rows, own, v_weight, q_weight, parcels, step_v, step_q, new_v, new_q, copy_v, copy_q, units,
    rate, *, rank, v_cols, q_cols, entries
):
    cols = v_cols + q_cols

    @pl.when(pl.program_id(0) == 0)
    def _():
        tail = rows[:, cols // 128 * 128 :].astype(jnp.float32)
        lane = lax.broadcasted_iota(jnp.int32, tail.shape, 1) + cols // 128 * 128
        total = jnp.sum(jnp.where((lane >= cols) & (lane < cols + 3), tail, 0.0), keepdims=True)
        scale = lax.rsqrt(total / entries + 1e-06)
        rate[...] = jnp.broadcast_to(learn_rate * scale, rate.shape)
        units[:rank, :v_cols] = rows[:, :v_cols]
        units[rank:, :v_cols] = jnp.zeros((rank, v_cols), units.dtype)
        units[:rank, v_cols:] = jnp.zeros((rank, q_cols), units.dtype)
        units[rank:, v_cols:] = rows[:, v_cols:cols]
        step = scale * jnp.dot(
            own[:, : 2 * rank], units[...], preferred_element_type=jnp.float32
        )
        step_v[...] = step[:, :v_cols]
        step_q[...] = step[:, v_cols:]
        new_v[...] = v_weight[...] - learn_rate * step[:, :v_cols]
        new_q[...] = q_weight[...] - learn_rate * step[:, v_cols:]

    to_v, from_q = min(rank + -rank % 128, 2 * rank), rank // 128 * 128
    weights = parcels[:, 2 * rank :].astype(jnp.float32)
    step = jnp.dot(parcels[:, :to_v], units[:to_v, :v_cols], preferred_element_type=jnp.float32)
    copy_v[...] = (weights[:, :v_cols] - rate[:, :v_cols] * step).astype(jnp.bfloat16)
    step = jnp.dot(
        parcels[:, from_q : 2 * rank], units[from_q:, v_cols:], preferred_element_type=jnp.float32
    )
    copy_q[...] = (weights[:, v_cols:] - rate[:, v_cols:] * step).astype(jnp.bfloat16).T


def on_device(
    inputs,
    query_cot,
    value_cot,
    query_factor,
    value_factor,
    query_weight,
    value_weight,
    query_first,
    query_second,
    value_first,
    value_second,
):
    sizes = tuple(lax.axis_size(a) for a in FS)
    n0, n1, n2 = sizes
    tp = lax.axis_size("tp")
    own, rank = query_factor.shape
    q_cols = query_cot.shape[1]
    v_cols = value_cot.shape[1]
    cols = q_cols + v_cols
    width = rank // tp
    whole = rank * own
    bf16, f32 = jnp.bfloat16, jnp.float32
    shape = jax.ShapeDtypeStruct
    vmem = pl.BlockSpec(memory_space=pltpu.VMEM)
    smem = pl.BlockSpec(memory_space=pltpu.SMEM)
    near_core = lambda a: pltpu.with_memory_space_constraint(a, pltpu.VMEM)
    at = lax.axis_index("tp").astype(jnp.int32).reshape(1)

    parcel, spread = pl.pallas_call(
        lambda *refs: pack_kernel(*refs, sizes=sizes, width=width),
        in_specs=[smem] + [vmem] * 4,
        out_specs=[vmem] * 2,
        out_shape=[shape((own, 2 * rank + cols), bf16), pltpu.VMEM((n0, own, 2 * width), bf16)],
        name="pack",
    )(at, value_factor, query_factor, value_weight, query_weight)
    parcels = lax.all_gather(parcel, FS, axis=0, tiled=True)

    near = lax.all_to_all(spread, "fs_0", 0, 0, tiled=True)
    near = sent_to_all(near, "fs_1")
    near = sent_to_all(near, "fs_2")
    share = near.transpose(2, 1, 0, 3, 4).reshape(-1, 2 * width)
    proj = lax.dot_general(
        share, inputs, (((0,), (1,)), ((), ())), preferred_element_type=f32
    ).astype(bf16)
    proj = lax.all_gather(proj, "tp", axis=0, tiled=True)

    chunks = v_cols // 128
    lines = n0 * (chunks + 1) + n0 // 2
    lines += -lines % 8
    blocks = pl.pallas_call(
        lambda *refs: terms_kernel(*refs, n0=n0, width=width),
        in_specs=[vmem] * 3,
        out_specs=vmem,
        out_shape=pltpu.VMEM((n1 * n2, lines, 128), bf16),
        scratch_shapes=[
            pltpu.VMEM((rank, v_cols), f32),
            pltpu.VMEM((rank, q_cols), f32),
            pltpu.VMEM((n1 * n2, lines, 128), f32),
        ],
        name="terms",
    )(near_core(proj), near_core(value_cot), near_core(query_cot.T))
    blocks = lax.all_to_all(blocks, ("fs_1", "fs_2"), 0, 0, tiled=True)
    term = pl.pallas_call(
        lambda *refs: fold_kernel(*refs, n0=n0, chunks=chunks),
        in_specs=[vmem],
        out_specs=vmem,
        out_shape=pltpu.VMEM((n0, 8, 128), f32),
        scratch_shapes=[pltpu.VMEM((lines, 128), f32)],
        name="fold",
    )(near_core(blocks))
    term = lax.all_to_all(term, "fs_0", 0, 0, tiled=True)
    first_v, second_v, first_q, second_q, spread = pl.pallas_call(
        moments_kernel,
        in_specs=[vmem] * 5,
        out_specs=[vmem] * 5,
        out_shape=[shape((1, v_cols), f32)] * 2
        + [shape((1, q_cols), f32)] * 2
        + [pltpu.VMEM((n1 * tp, 8, 128), bf16)],
        name="moments",
    )(
        near_core(term),
        near_core(value_first),
        near_core(value_second),
        near_core(query_first),
        near_core(query_second),
    )

    blocks = lax.all_to_all(spread, ("fs_1", "tp"), 0, 0, tiled=True)
    lines = -(-(cols + 3) // 128)
    spread = pl.pallas_call(
        lambda *refs: regroup_kernel(*refs, cols=cols),
        in_specs=[smem, vmem],
        out_specs=vmem,
        out_shape=pltpu.VMEM((n0, n1, lines * 128), bf16),
        name="regroup",
    )(at, near_core(blocks.reshape(n1, tp, 8, 128)))
    rows = lax.all_to_all(spread, "fs_0", 0, 0, tiled=True).reshape(n0 * n1, -1)
    rows = sent_to_all(rows, "fs_2").reshape(rank, -1)

    steps = 2
    block = whole // steps
    fixed = lambda *s: pl.BlockSpec(s, lambda i: (0, 0))
    step_v, step_q, new_v, new_q, copy_v, copy_q = pl.pallas_call(
        lambda *refs: update_kernel(
            *refs, rank=rank, v_cols=v_cols, q_cols=q_cols, entries=rank * cols * tp
        ),
        grid=(steps,),
        in_specs=[
            fixed(rank, lines * 128),
            fixed(own, 2 * rank + cols),
            fixed(own, v_cols),
            fixed(own, q_cols),
            pl.BlockSpec((block, 2 * rank + cols), lambda i: (i, 0)),
        ],
        out_specs=[
            fixed(own, v_cols),
            fixed(own, q_cols),
            fixed(own, v_cols),
            fixed(own, q_cols),
            pl.BlockSpec((block, v_cols), lambda i: (i, 0)),
            pl.BlockSpec((q_cols, block), lambda i: (0, i)),
        ],
        out_shape=[
            shape((own, v_cols), f32),
            shape((own, q_cols), f32),
            shape((own, v_cols), f32),
            shape((own, q_cols), f32),
            shape((whole, v_cols), bf16),
            shape((q_cols, whole), bf16),
        ],
        scratch_shapes=[pltpu.VMEM((2 * rank, cols), bf16), pltpu.VMEM((1, cols), f32)],
        name="update",
    )(near_core(rows), parcel, value_weight, query_weight, parcels)
    return (step_q, step_v, new_q, new_v, first_q, second_q, first_v, second_v, copy_q.T, copy_v)


def solution(mesh):
    split = Mesh(mesh.devices.reshape(12, 8, 2, mesh.shape["tp"]), ("fs_0", "fs_1", "fs_2", "tp"))
    return jax.shard_map(
        on_device,
        mesh=split,
        in_specs=(
            P(FS, None),
            P(FS, "tp"),
            P(FS, "tp"),
            P(FS, None),
            P(FS, None),
            P(FS, "tp"),
            P(FS, "tp"),
            P(FS, "tp"),
            P(FS, "tp"),
            P(FS, "tp"),
            P(FS, "tp"),
        ),
        out_specs=(
            P(FS, "tp"),
            P(FS, "tp"),
            P(FS, "tp"),
            P(FS, "tp"),
            P(FS, "tp"),
            P(FS, "tp"),
            P(FS, "tp"),
            P(FS, "tp"),
            P(None, "tp"),
            P(None, "tp"),
        ),
        check_vma=False,
    )
```

```python
import math

import jax
import jax.numpy as jnp
from jax import lax
from jax.experimental import pallas as pl
from jax.experimental.pallas import tpu as pltpu
from jax.sharding import Mesh
from jax.sharding import PartitionSpec as P

FS = ("fs_0", "fs_1", "fs_2")


first_decay = 0.9
second_decay = 0.99
small_eps = 1e-08
learn_rate = 0.01


def sent_to_all(value, axis):
    size = lax.axis_size(axis)
    return lax.all_to_all(
        jnp.broadcast_to(value[None], (size, *value.shape)), axis, 0, 0, tiled=True
    )


def shift_of(size):
    shift = int(math.log2(size))
    assert 1 << shift == size
    return shift


def pack_kernel(v_factor, q_factor, v_weight, q_weight, parcel):
    parcel[...] = jnp.concatenate(
        [
            v_factor[...],
            q_factor[...],
            v_weight[...].astype(jnp.bfloat16),
            q_weight[...].astype(jnp.bfloat16),
        ],
        axis=1,
    )


def share_kernel(at, v_factor, q_factor, spread, *, sizes, width):
    rank = v_factor.shape[1]
    n0, n1, n2 = sizes
    row = lax.broadcasted_iota(jnp.int32, (rank, width), 0)
    place = (row & (n1 * n2 - 1)) * n0 + (row >> shift_of(n1 * n2))
    col = lax.broadcasted_iota(jnp.int32, (rank, width), 1)
    mine = (place == col + at[0] * width).astype(jnp.float32).astype(jnp.bfloat16)
    parts = [
        jnp.dot(f[...], mine, preferred_element_type=jnp.float32).astype(jnp.bfloat16)
        for f in (v_factor, q_factor)
    ]
    spread[...] = jnp.broadcast_to(jnp.concatenate(parts, axis=1)[None], spread.shape)


def terms_kernel(proj, v_cot, q_cot, blocks, term_v, term_q, wide, *, n0, width):
    rank, v_cols = term_v.shape
    tp = rank // width
    parts = [proj[2 * width * t : 2 * width * (t + 1), :] for t in range(tp)]
    proj_v = jnp.concatenate([p[:width] for p in parts], axis=0)
    proj_q = jnp.concatenate([p[width:] for p in parts], axis=0)
    term_v[...] = jnp.dot(proj_v, v_cot[...], preferred_element_type=jnp.float32)
    term_q[...] = lax.dot_general(
        proj_q, q_cot[...], (((1,), (1,)), ((), ())), preferred_element_type=jnp.float32
    )
    chunks, half = v_cols // 128, n0 // 2
    wide[...] = jnp.zeros(wide.shape, jnp.float32)
    for b in range(rank // n0):
        for k in range(chunks):
            wide[b, n0 * k : n0 * (k + 1), :] = term_v[
                n0 * b : n0 * (b + 1), 128 * k : 128 * (k + 1)
            ]
        wide[b, n0 * chunks : n0 * (chunks + 1), :] = term_q[n0 * b : n0 * (b + 1), :128]
        rest = jnp.concatenate(
            [term_q[n0 * b : n0 * b + half, 128:], term_q[n0 * b + half : n0 * (b + 1), 128:]],
            axis=1,
        )
        wide[b, n0 * (chunks + 1) : n0 * (chunks + 1) + half, :] = rest
    blocks[...] = wide[...].astype(jnp.bfloat16)


def fold_kernel(blocks, rows, wide, *, n0, chunks):
    wide[...] = jnp.sum(blocks[...].astype(jnp.float32), axis=0)
    half = n0 // 2
    rows[...] = jnp.zeros(rows.shape, jnp.float32)
    for r in range(n0):
        for k in range(chunks + 1):
            rows[r, k : k + 1, :] = wide[n0 * k + r : n0 * k + r + 1, :]
        line = n0 * (chunks + 1) + r % half
        rest = wide[line : line + 1, :]
        if r >= half:
            rest = jnp.concatenate([rest[:, 64:], rest[:, :64]], axis=1)
        rows[r, chunks + 1 : chunks + 2, :] = rest


def pieces_of(value):
    high = value.astype(jnp.bfloat16).astype(jnp.float32)
    middle = (value - high).astype(jnp.bfloat16).astype(jnp.float32)
    return high, middle, value - high - middle


def with_pieces(value, block, at):
    lane = lax.broadcasted_iota(jnp.int32, block.shape, 1)
    for k, piece in enumerate(pieces_of(value)):
        block = jnp.where(lane == at + k, piece, block)
    return block


def moments(old_first, old_second, gradient):
    first = first_decay * old_first + (1.0 - first_decay) * gradient
    second = second_decay * old_second + (1.0 - second_decay) * gradient * gradient
    unit = first / (jnp.sqrt(second) + small_eps)
    return (first, second, unit)


def moments_kernel(terms, v_first, v_second, q_first, q_second, *outs):
    first_v, second_v, first_q, second_q, spread = outs
    v_cols, q_cols = v_first.shape[1], q_first.shape[1]
    gradient = jnp.sum(terms[...], axis=0)
    gradient = jnp.concatenate(
        [gradient[k : k + 1] for k in range(v_cols // 128 + 1)]
        + [gradient[v_cols // 128 + 1 : v_cols // 128 + 2, : q_cols - 128]],
        axis=1,
    )
    first_v[...], second_v[...], unit_v = moments(v_first[...], v_second[...], gradient[:, :v_cols])
    first_q[...], second_q[...], unit_q = moments(q_first[...], q_second[...], gradient[:, v_cols:])
    squares = jnp.sum(unit_v * unit_v, axis=1, keepdims=True)
    squares += jnp.sum(unit_q * unit_q, axis=1, keepdims=True)
    cols = gradient.shape[1]
    lines = -(-(cols + 3) // 128)
    row = jnp.concatenate(
        [unit_v, unit_q, jnp.zeros((1, lines * 128 - cols), jnp.float32)], axis=1
    )
    row = with_pieces(squares, row, cols)
    block = jnp.concatenate(
        [row[:, 128 * k : 128 * (k + 1)] for k in range(lines)]
        + [jnp.zeros((spread.shape[1] - lines, 128), jnp.float32)],
        axis=0,
    ).astype(jnp.bfloat16)
    spread[...] = jnp.broadcast_to(block[None], spread.shape)


def regroup_kernel(at, blocks, spread, *, cols):
    n1, tp = blocks.shape[:2]
    lines = spread.shape[2] // 128
    last, begin = cols // 128, cols % 128
    ends = blocks[:, :, last, :].astype(jnp.float32)
    ends = jnp.sum(ends, axis=1)
    lane = lax.broadcasted_iota(jnp.int32, ends.shape, 1)
    squares = jnp.where((lane >= begin) & (lane < begin + 3), ends, 0.0)
    squares = jnp.sum(squares, axis=1, keepdims=True)
    own = blocks[:, at[0], :, :].astype(jnp.float32)
    parts = [own[:, k, :] for k in range(lines)]
    parts[last] = with_pieces(squares, parts[last], begin)
    rows = jnp.concatenate(parts, axis=1).astype(jnp.bfloat16)
    spread[...] = jnp.broadcast_to(rows[None], spread.shape)


def finish_kernel(
    rows, v_factor, q_factor, v_weight, q_weight, step_v, step_q, new_v, new_q, units, rate,
    *, sizes, v_cols, entries
):
    rank = rows.shape[0]
    cols = units.shape[1]
    n0, n1, n2 = sizes
    tail = rows[:, cols // 128 * 128 :].astype(jnp.float32)
    lane = lax.broadcasted_iota(jnp.int32, tail.shape, 1) + cols // 128 * 128
    total = jnp.sum(jnp.where((lane >= cols) & (lane < cols + 3), tail, 0.0), keepdims=True)
    scale = lax.rsqrt(total / entries + 1e-06)
    rate[...] = jnp.broadcast_to(learn_rate * scale, rate.shape)
    row = lax.broadcasted_iota(jnp.int32, (rank, rank), 0)
    far = row >> shift_of(n1 * n2)
    place = (row & (n2 - 1)) * (n0 * n1) + far * n1 + ((row >> shift_of(n2)) & (n1 - 1))
    turn = place == lax.broadcasted_iota(jnp.int32, (rank, rank), 1)
    turn = turn.astype(jnp.float32).astype(jnp.bfloat16)
    turned = jnp.dot(turn, rows[...], preferred_element_type=jnp.float32).astype(jnp.bfloat16)
    units[:rank, :v_cols] = turned[:, :v_cols]
    units[rank:, :v_cols] = jnp.zeros((rank, v_cols), units.dtype)
    units[:rank, v_cols:] = jnp.zeros((rank, cols - v_cols), units.dtype)
    units[rank:, v_cols:] = turned[:, v_cols:cols]
    step = scale * jnp.dot(v_factor[...], turned[:, :v_cols], preferred_element_type=jnp.float32)
    step_v[...] = step
    new_v[...] = v_weight[...] - learn_rate * step
    step = scale * jnp.dot(
        q_factor[...], turned[:, v_cols:cols], preferred_element_type=jnp.float32
    )
    step_q[...] = step
    new_q[...] = q_weight[...] - learn_rate * step


def copies_kernel(units, rate, parcels, copy_v, copy_q, *, rank, v_cols):
    to_v, from_q = min(rank + -rank % 128, 2 * rank), rank // 128 * 128
    weights = parcels[:, 2 * rank :].astype(jnp.float32)
    step = jnp.dot(parcels[:, :to_v], units[:to_v, :v_cols], preferred_element_type=jnp.float32)
    copy_v[...] = (weights[:, :v_cols] - rate[:, :v_cols] * step).astype(jnp.bfloat16)
    step = jnp.dot(
        parcels[:, from_q : 2 * rank], units[from_q:, v_cols:], preferred_element_type=jnp.float32
    )
    copy_q[...] = (weights[:, v_cols:] - rate[:, v_cols:] * step).astype(jnp.bfloat16).T


def on_device(
    inputs,
    query_cot,
    value_cot,
    query_factor,
    value_factor,
    query_weight,
    value_weight,
    query_first,
    query_second,
    value_first,
    value_second,
):
    sizes = tuple(lax.axis_size(a) for a in FS)
    n0, n1, n2 = sizes
    tp = lax.axis_size("tp")
    own, rank = query_factor.shape
    q_cols = query_cot.shape[1]
    v_cols = value_cot.shape[1]
    cols = q_cols + v_cols
    width = rank // tp
    whole = rank * own
    bf16, f32 = jnp.bfloat16, jnp.float32
    shape = jax.ShapeDtypeStruct
    vmem = pl.BlockSpec(memory_space=pltpu.VMEM)
    smem = pl.BlockSpec(memory_space=pltpu.SMEM)
    near_core = lambda a: pltpu.with_memory_space_constraint(a, pltpu.VMEM)
    at = lax.axis_index("tp").astype(jnp.int32).reshape(1)

    parcel = pl.pallas_call(
        pack_kernel,
        in_specs=[vmem] * 4,
        out_specs=vmem,
        out_shape=shape((own, 2 * rank + cols), bf16),
        name="pack",
    )(value_factor, query_factor, value_weight, query_weight)
    parcels = lax.all_gather(parcel, FS, axis=0, tiled=True)
    spread = pl.pallas_call(
        lambda *refs: share_kernel(*refs, sizes=sizes, width=width),
        in_specs=[smem] + [vmem] * 2,
        out_specs=vmem,
        out_shape=pltpu.VMEM((n0, own, 2 * width), bf16),
        name="share",
    )(at, value_factor, query_factor)

    near = lax.all_to_all(spread, "fs_0", 0, 0, tiled=True)
    near = sent_to_all(near, "fs_1")
    near = sent_to_all(near, "fs_2")
    share = near.transpose(2, 1, 0, 3, 4).reshape(-1, 2 * width)
    proj = lax.dot_general(
        share, inputs, (((0,), (1,)), ((), ())), preferred_element_type=f32
    ).astype(bf16)
    proj = lax.all_gather(proj, "tp", axis=0, tiled=True)

    chunks = v_cols // 128
    lines = n0 * (chunks + 1) + n0 // 2
    lines += -lines % 8
    blocks = pl.pallas_call(
        lambda *refs: terms_kernel(*refs, n0=n0, width=width),
        in_specs=[vmem] * 3,
        out_specs=vmem,
        out_shape=pltpu.VMEM((n1 * n2, lines, 128), bf16),
        scratch_shapes=[
            pltpu.VMEM((rank, v_cols), f32),
            pltpu.VMEM((rank, q_cols), f32),
            pltpu.VMEM((n1 * n2, lines, 128), f32),
        ],
        name="terms",
    )(near_core(proj), near_core(value_cot), near_core(query_cot.T))
    blocks = lax.all_to_all(blocks, ("fs_1", "fs_2"), 0, 0, tiled=True)
    term = pl.pallas_call(
        lambda *refs: fold_kernel(*refs, n0=n0, chunks=chunks),
        in_specs=[vmem],
        out_specs=vmem,
        out_shape=pltpu.VMEM((n0, 8, 128), f32),
        scratch_shapes=[pltpu.VMEM((lines, 128), f32)],
        name="fold",
    )(near_core(blocks))
    term = lax.all_to_all(term, "fs_0", 0, 0, tiled=True)
    first_v, second_v, first_q, second_q, spread = pl.pallas_call(
        moments_kernel,
        in_specs=[vmem] * 5,
        out_specs=[vmem] * 5,
        out_shape=[shape((1, v_cols), f32)] * 2
        + [shape((1, q_cols), f32)] * 2
        + [pltpu.VMEM((n1 * tp, 8, 128), bf16)],
        name="moments",
    )(
        near_core(term),
        near_core(value_first),
        near_core(value_second),
        near_core(query_first),
        near_core(query_second),
    )

    blocks = lax.all_to_all(spread, ("fs_1", "tp"), 0, 0, tiled=True)
    lines = -(-(cols + 3) // 128)
    spread = pl.pallas_call(
        lambda *refs: regroup_kernel(*refs, cols=cols),
        in_specs=[smem, vmem],
        out_specs=vmem,
        out_shape=pltpu.VMEM((n0, n1, lines * 128), bf16),
        name="regroup",
    )(at, near_core(blocks.reshape(n1, tp, 8, 128)))
    rows = lax.all_to_all(spread, "fs_0", 0, 0, tiled=True).reshape(n0 * n1, -1)
    rows = sent_to_all(rows, "fs_2").reshape(rank, -1)

    step_v, step_q, new_v, new_q, units, rate = pl.pallas_call(
        lambda *refs: finish_kernel(*refs, sizes=sizes, v_cols=v_cols, entries=rank * cols * tp),
        in_specs=[vmem] * 5,
        out_specs=[vmem] * 6,
        out_shape=[
            shape((own, v_cols), f32),
            shape((own, q_cols), f32),
            shape((own, v_cols), f32),
            shape((own, q_cols), f32),
            pltpu.VMEM((2 * rank, cols), bf16),
            pltpu.VMEM((1, cols), f32),
        ],
        name="finish",
    )(
        near_core(rows),
        near_core(value_factor),
        near_core(query_factor),
        near_core(value_weight),
        near_core(query_weight),
    )

    steps = 2
    block = whole // steps
    copy_v, copy_q = pl.pallas_call(
        lambda *refs: copies_kernel(*refs, rank=rank, v_cols=v_cols),
        grid=(steps,),
        in_specs=[vmem, vmem, pl.BlockSpec((block, 2 * rank + cols), lambda i: (i, 0))],
        out_specs=[
            pl.BlockSpec((block, v_cols), lambda i: (i, 0)),
            pl.BlockSpec((q_cols, block), lambda i: (0, i)),
        ],
        out_shape=[shape((whole, v_cols), bf16), shape((q_cols, whole), bf16)],
        name="copies",
    )(near_core(units), near_core(rate), parcels)
    return (step_q, step_v, new_q, new_v, first_q, second_q, first_v, second_v, copy_q.T, copy_v)


def solution(mesh):
    split = Mesh(mesh.devices.reshape(12, 8, 2, mesh.shape["tp"]), ("fs_0", "fs_1", "fs_2", "tp"))
    return jax.shard_map(
        on_device,
        mesh=split,
        in_specs=(
            P(FS, None),
            P(FS, "tp"),
            P(FS, "tp"),
            P(FS, None),
            P(FS, None),
            P(FS, "tp"),
            P(FS, "tp"),
            P(FS, "tp"),
            P(FS, "tp"),
            P(FS, "tp"),
            P(FS, "tp"),
        ),
        out_specs=(
            P(FS, "tp"),
            P(FS, "tp"),
            P(FS, "tp"),
            P(FS, "tp"),
            P(FS, "tp"),
            P(FS, "tp"),
            P(FS, "tp"),
            P(FS, "tp"),
            P(None, "tp"),
            P(None, "tp"),
        ),
        check_vma=False,
    )
```

```python
import math

import jax
import jax.numpy as jnp
from jax import lax
from jax.experimental import pallas as pl
from jax.experimental.pallas import tpu as pltpu
from jax.sharding import Mesh
from jax.sharding import PartitionSpec as P

FS = ("fs_0", "fs_1", "fs_2")


first_decay = 0.9
second_decay = 0.99
small_eps = 1e-08
learn_rate = 0.01


def sent_to_all(value, axis):
    size = lax.axis_size(axis)
    return lax.all_to_all(
        jnp.broadcast_to(value[None], (size, *value.shape)), axis, 0, 0, tiled=True
    )


def shift_of(size):
    shift = int(math.log2(size))
    assert 1 << shift == size
    return shift


def pack_kernel(v_factor, q_factor, v_weight, q_weight, spread):
    parcel = jnp.concatenate(
        [
            v_factor[...],
            q_factor[...],
            v_weight[...].astype(jnp.bfloat16),
            q_weight[...].astype(jnp.bfloat16),
        ],
        axis=1,
    )
    spread[...] = jnp.broadcast_to(parcel[None], spread.shape)


def in_lines(share):
    rows, wide = share.shape
    if wide != 96:
        return share
    top = rows * 3 // 4
    extra = [share[top:, 32 * k : 32 * (k + 1)] for k in range(3)]
    return jnp.concatenate([share[:top], jnp.concatenate(extra, axis=0)], axis=1)


def out_of_lines(lines, wide):
    if wide != 96:
        return lines
    part = lines.shape[1] // 3
    extra = [lines[:, part * k : part * (k + 1), 96:] for k in range(3)]
    return jnp.concatenate([lines[:, :, :96], jnp.concatenate(extra, axis=2)], axis=1)


def share_kernel(at, factors, spread, *, sizes, width):
    n0, n1, n2 = sizes
    rank = factors.shape[2] // 2
    row = lax.broadcasted_iota(jnp.int32, (2 * rank, 2 * width), 0)
    col = lax.broadcasted_iota(jnp.int32, (2 * rank, 2 * width), 1)
    of_q = row >= rank
    row = jnp.where(of_q, row - rank, row)
    place = (row & (n1 * n2 - 1)) * n0 + (row >> shift_of(n1 * n2))
    mine = (of_q == (col >= width)) & (
        place == jnp.where(col >= width, col - width, col) + at[0] * width
    )
    mine = mine.astype(jnp.float32).astype(jnp.bfloat16)
    whole = factors[...].reshape(-1, 2 * rank)
    share = jnp.dot(whole, mine, preferred_element_type=jnp.float32)
    spread[...] = jnp.broadcast_to(in_lines(share).astype(jnp.bfloat16)[None], spread.shape)


def project_kernel(lines, inputs, proj, share):
    n0, n1, n2, own, wide = share.shape
    for c in range(n2):
        share[:, :, c, :, :] = out_of_lines(lines[c], wide).reshape(n0, n1, own, wide)
    factors = share[...].reshape(-1, wide)
    sums = jnp.dot(inputs[...], factors, preferred_element_type=jnp.float32)
    proj[...] = sums.astype(jnp.bfloat16).T


def terms_kernel(proj, v_cot, q_cot, blocks, term_v, term_q, wide, *, n0, width):
    rank, v_cols = term_v.shape
    tp = rank // width
    parts = [proj[2 * width * t : 2 * width * (t + 1), :] for t in range(tp)]
    proj_v = jnp.concatenate([p[:width] for p in parts], axis=0)
    proj_q = jnp.concatenate([p[width:] for p in parts], axis=0)
    term_v[...] = jnp.dot(proj_v, v_cot[...], preferred_element_type=jnp.float32)
    term_q[...] = lax.dot_general(
        proj_q, q_cot[...], (((1,), (1,)), ((), ())), preferred_element_type=jnp.float32
    )
    chunks, half = v_cols // 128, n0 // 2
    wide[...] = jnp.zeros(wide.shape, jnp.float32)
    for b in range(rank // n0):
        for k in range(chunks):
            wide[b, n0 * k : n0 * (k + 1), :] = term_v[
                n0 * b : n0 * (b + 1), 128 * k : 128 * (k + 1)
            ]
        wide[b, n0 * chunks : n0 * (chunks + 1), :] = term_q[n0 * b : n0 * (b + 1), :128]
        rest = jnp.concatenate(
            [term_q[n0 * b : n0 * b + half, 128:], term_q[n0 * b + half : n0 * (b + 1), 128:]],
            axis=1,
        )
        wide[b, n0 * (chunks + 1) : n0 * (chunks + 1) + half, :] = rest
    blocks[...] = wide[...].astype(jnp.bfloat16)


def fold_kernel(blocks, rows, wide, *, n0, chunks):
    wide[...] = jnp.sum(blocks[...].astype(jnp.float32), axis=0)
    half = n0 // 2
    rows[...] = jnp.zeros(rows.shape, jnp.float32)
    for r in range(n0):
        for k in range(chunks + 1):
            rows[r, k : k + 1, :] = wide[n0 * k + r : n0 * k + r + 1, :]
        line = n0 * (chunks + 1) + r % half
        rest = wide[line : line + 1, :]
        if r >= half:
            rest = jnp.concatenate([rest[:, 64:], rest[:, :64]], axis=1)
        rows[r, chunks + 1 : chunks + 2, :] = rest


def pieces_of(value):
    high = value.astype(jnp.bfloat16).astype(jnp.float32)
    middle = (value - high).astype(jnp.bfloat16).astype(jnp.float32)
    return high, middle, value - high - middle


def with_pieces(value, block, at):
    lane = lax.broadcasted_iota(jnp.int32, block.shape, 1)
    for k, piece in enumerate(pieces_of(value)):
        block = jnp.where(lane == at + k, piece, block)
    return block


def moments(old_first, old_second, gradient):
    first = first_decay * old_first + (1.0 - first_decay) * gradient
    second = second_decay * old_second + (1.0 - second_decay) * gradient * gradient
    unit = first / (jnp.sqrt(second) + small_eps)
    return (first, second, unit)


def moments_kernel(terms, v_first, v_second, q_first, q_second, *outs):
    first_v, second_v, first_q, second_q, spread = outs
    v_cols, q_cols = v_first.shape[1], q_first.shape[1]
    gradient = jnp.sum(terms[...], axis=0)
    gradient = jnp.concatenate(
        [gradient[k : k + 1] for k in range(v_cols // 128 + 1)]
        + [gradient[v_cols // 128 + 1 : v_cols // 128 + 2, : q_cols - 128]],
        axis=1,
    )
    first_v[...], second_v[...], unit_v = moments(v_first[...], v_second[...], gradient[:, :v_cols])
    first_q[...], second_q[...], unit_q = moments(q_first[...], q_second[...], gradient[:, v_cols:])
    squares = jnp.sum(unit_v * unit_v, axis=1, keepdims=True)
    squares += jnp.sum(unit_q * unit_q, axis=1, keepdims=True)
    cols = gradient.shape[1]
    lines = -(-(cols + 3) // 128)
    row = jnp.concatenate(
        [unit_v, unit_q, jnp.zeros((1, lines * 128 - cols), jnp.float32)], axis=1
    )
    row = with_pieces(squares, row, cols)
    block = jnp.concatenate(
        [row[:, 128 * k : 128 * (k + 1)] for k in range(lines)]
        + [jnp.zeros((spread.shape[1] - lines, 128), jnp.float32)],
        axis=0,
    ).astype(jnp.bfloat16)
    spread[...] = jnp.broadcast_to(block[None], spread.shape)


def regroup_kernel(at, blocks, spread, *, cols):
    n1, tp = blocks.shape[:2]
    lines = spread.shape[2] // 128
    last, begin = cols // 128, cols % 128
    ends = blocks[:, :, last, :].astype(jnp.float32)
    ends = jnp.sum(ends, axis=1)
    lane = lax.broadcasted_iota(jnp.int32, ends.shape, 1)
    squares = jnp.where((lane >= begin) & (lane < begin + 3), ends, 0.0)
    squares = jnp.sum(squares, axis=1, keepdims=True)
    own = blocks[:, at[0], :, :].astype(jnp.float32)
    parts = [own[:, k, :] for k in range(lines)]
    parts[last] = with_pieces(squares, parts[last], begin)
    rows = jnp.concatenate(parts, axis=1).astype(jnp.bfloat16)
    spread[...] = jnp.broadcast_to(rows[None], spread.shape)


def finish_kernel(
    rows, v_factor, q_factor, v_weight, q_weight, step_v, step_q, new_v, new_q, units, rate,
    *, sizes, v_cols, entries
):
    rank = rows.shape[0]
    cols = units.shape[1]
    n0, n1, n2 = sizes
    tail = rows[:, cols // 128 * 128 :].astype(jnp.float32)
    lane = lax.broadcasted_iota(jnp.int32, tail.shape, 1) + cols // 128 * 128
    total = jnp.sum(jnp.where((lane >= cols) & (lane < cols + 3), tail, 0.0), keepdims=True)
    scale = lax.rsqrt(total / entries + 1e-06)
    rate[...] = jnp.broadcast_to(learn_rate * scale, rate.shape)
    row = lax.broadcasted_iota(jnp.int32, (rank, rank), 0)
    far = row >> shift_of(n1 * n2)
    place = (row & (n2 - 1)) * (n0 * n1) + far * n1 + ((row >> shift_of(n2)) & (n1 - 1))
    turn = place == lax.broadcasted_iota(jnp.int32, (rank, rank), 1)
    turn = turn.astype(jnp.float32).astype(jnp.bfloat16)
    turned = jnp.dot(turn, rows[...], preferred_element_type=jnp.float32).astype(jnp.bfloat16)
    units[:rank, :v_cols] = turned[:, :v_cols]
    units[rank:, :v_cols] = jnp.zeros((rank, v_cols), units.dtype)
    units[:rank, v_cols:] = jnp.zeros((rank, cols - v_cols), units.dtype)
    units[rank:, v_cols:] = turned[:, v_cols:cols]
    step = scale * jnp.dot(v_factor[...], turned[:, :v_cols], preferred_element_type=jnp.float32)
    step_v[...] = step
    new_v[...] = v_weight[...] - learn_rate * step
    step = scale * jnp.dot(
        q_factor[...], turned[:, v_cols:cols], preferred_element_type=jnp.float32
    )
    step_q[...] = step
    new_q[...] = q_weight[...] - learn_rate * step


def copies_kernel(units, rate, parcels, copy_v, copy_q, turned, *, rank, v_cols):
    to_v, from_q = min(rank + -rank % 128, 2 * rank), rank // 128 * 128
    block, n1, n2, own, q_cols = turned.shape
    part = parcels[pl.ds(pl.program_id(0) * block, block)].reshape(-1, parcels.shape[-1])
    weights = part[:, 2 * rank :].astype(jnp.float32)
    step = jnp.dot(part[:, :to_v], units[:to_v, :v_cols], preferred_element_type=jnp.float32)
    new = (weights[:, :v_cols] - rate[:, :v_cols] * step).astype(jnp.bfloat16)
    new = new.reshape(block, n2, n1, own, v_cols)
    for c in range(n2):
        copy_v[:, :, c, :, :] = new[:, c]
    step = jnp.dot(
        part[:, from_q : 2 * rank], units[from_q:, v_cols:], preferred_element_type=jnp.float32
    )
    new = (weights[:, v_cols:] - rate[:, v_cols:] * step).astype(jnp.bfloat16)
    new = new.reshape(block, n2, n1, own, q_cols)
    for c in range(n2):
        turned[:, :, c, :, :] = new[:, c]
    copy_q[...] = turned[...].reshape(-1, q_cols).T


def on_device(
    inputs,
    query_cot,
    value_cot,
    query_factor,
    value_factor,
    query_weight,
    value_weight,
    query_first,
    query_second,
    value_first,
    value_second,
):
    sizes = tuple(lax.axis_size(a) for a in FS)
    n0, n1, n2 = sizes
    tp = lax.axis_size("tp")
    own, rank = query_factor.shape
    q_cols = query_cot.shape[1]
    v_cols = value_cot.shape[1]
    cols = q_cols + v_cols
    width = rank // tp
    whole = rank * own
    bf16, f32 = jnp.bfloat16, jnp.float32
    shape = jax.ShapeDtypeStruct
    vmem = pl.BlockSpec(memory_space=pltpu.VMEM)
    smem = pl.BlockSpec(memory_space=pltpu.SMEM)
    small = pltpu.CompilerParams(vmem_limit_bytes=16 * 1024 * 1024)
    waits = pl.CostEstimate(flops=20_000_000_000, transcendentals=0, bytes_accessed=1_000_000)
    near_core = lambda a: pltpu.with_memory_space_constraint(a, pltpu.VMEM)
    at = lax.axis_index("tp").astype(jnp.int32).reshape(1)

    parts = 2 * rank + cols
    spread = pl.pallas_call(
        pack_kernel,
        in_specs=[vmem] * 4,
        out_specs=vmem,
        out_shape=pltpu.VMEM((n1, own, parts), bf16),
        name="pack",
    )(value_factor, query_factor, value_weight, query_weight)
    near = lax.all_to_all(spread, "fs_1", 0, 0, tiled=True)
    parcels = lax.all_gather(near.reshape(n1 * own, parts), ("fs_0", "fs_2"), axis=0, tiled=True)

    lines = (n1 * own * 3 // 4, 128) if 2 * width == 96 else (n1 * own, 2 * width)
    spread = pl.pallas_call(
        lambda *refs: share_kernel(*refs, sizes=sizes, width=width),
        grid=(1,),
        in_specs=[smem, pl.BlockSpec((n1, own, 2 * rank), lambda i: (0, 0, 0))],
        out_specs=vmem,
        out_shape=pltpu.VMEM((n0, *lines), bf16),
        compiler_params=small,
        cost_estimate=waits,
        name="share",
    )(at, pltpu.with_memory_space_constraint(near, pltpu.HBM))
    near = lax.all_to_all(spread, "fs_0", 0, 0, tiled=True)
    near = sent_to_all(near, "fs_2").reshape(n2, n0, *lines)
    proj = pl.pallas_call(
        project_kernel,
        in_specs=[vmem] * 2,
        out_specs=vmem,
        out_shape=pltpu.VMEM((2 * width, inputs.shape[0]), bf16),
        scratch_shapes=[pltpu.VMEM((n0, n1, n2, own, 2 * width), bf16)],
        compiler_params=small,
        name="project",
    )(near_core(near), near_core(inputs))
    proj = lax.all_gather(proj, "tp", axis=0, tiled=True)

    chunks = v_cols // 128
    lines = n0 * (chunks + 1) + n0 // 2
    lines += -lines % 8
    blocks = pl.pallas_call(
        lambda *refs: terms_kernel(*refs, n0=n0, width=width),
        in_specs=[vmem] * 3,
        out_specs=vmem,
        out_shape=pltpu.VMEM((n1 * n2, lines, 128), bf16),
        scratch_shapes=[
            pltpu.VMEM((rank, v_cols), f32),
            pltpu.VMEM((rank, q_cols), f32),
            pltpu.VMEM((n1 * n2, lines, 128), f32),
        ],
        name="terms",
    )(near_core(proj), near_core(value_cot), near_core(query_cot.T))
    blocks = lax.all_to_all(blocks, ("fs_1", "fs_2"), 0, 0, tiled=True)
    term = pl.pallas_call(
        lambda *refs: fold_kernel(*refs, n0=n0, chunks=chunks),
        in_specs=[vmem],
        out_specs=vmem,
        out_shape=pltpu.VMEM((n0, 8, 128), f32),
        scratch_shapes=[pltpu.VMEM((lines, 128), f32)],
        name="fold",
    )(near_core(blocks))
    term = lax.all_to_all(term, "fs_0", 0, 0, tiled=True)
    first_v, second_v, first_q, second_q, spread = pl.pallas_call(
        moments_kernel,
        in_specs=[vmem] * 5,
        out_specs=[vmem] * 5,
        out_shape=[shape((1, v_cols), f32)] * 2
        + [shape((1, q_cols), f32)] * 2
        + [pltpu.VMEM((n1 * tp, 8, 128), bf16)],
        name="moments",
    )(
        near_core(term),
        near_core(value_first),
        near_core(value_second),
        near_core(query_first),
        near_core(query_second),
    )

    spread, parcels = lax.optimization_barrier((spread, parcels))
    blocks = lax.all_to_all(spread, ("fs_1", "tp"), 0, 0, tiled=True)
    lines = -(-(cols + 3) // 128)
    spread = pl.pallas_call(
        lambda *refs: regroup_kernel(*refs, cols=cols),
        in_specs=[smem, vmem],
        out_specs=vmem,
        out_shape=pltpu.VMEM((n0, n1, lines * 128), bf16),
        compiler_params=small,
        cost_estimate=waits,
        name="regroup",
    )(at, near_core(blocks.reshape(n1, tp, 8, 128)))
    rows = lax.all_to_all(spread, "fs_0", 0, 0, tiled=True).reshape(n0 * n1, -1)
    rows = sent_to_all(rows, "fs_2").reshape(rank, -1)

    step_v, step_q, new_v, new_q, units, rate = pl.pallas_call(
        lambda *refs: finish_kernel(*refs, sizes=sizes, v_cols=v_cols, entries=rank * cols * tp),
        in_specs=[vmem] * 5,
        out_specs=[vmem] * 6,
        out_shape=[
            shape((own, v_cols), f32),
            shape((own, q_cols), f32),
            shape((own, v_cols), f32),
            shape((own, q_cols), f32),
            pltpu.VMEM((2 * rank, cols), bf16),
            pltpu.VMEM((1, cols), f32),
        ],
        compiler_params=small,
        cost_estimate=waits,
        name="finish",
    )(
        near_core(rows),
        near_core(value_factor),
        near_core(query_factor),
        near_core(value_weight),
        near_core(query_weight),
    )

    steps = 4
    block = n0 // steps
    copy_v, copy_q = pl.pallas_call(
        lambda *refs: copies_kernel(*refs, rank=rank, v_cols=v_cols),
        grid=(steps,),
        in_specs=[
            vmem,
            vmem,
            vmem,
        ],
        out_specs=[
            pl.BlockSpec((block, n1, n2, own, v_cols), lambda i: (i, 0, 0, 0, 0)),
            pl.BlockSpec((q_cols, whole // steps), lambda i: (0, i)),
        ],
        out_shape=[shape((n0, n1, n2, own, v_cols), bf16), shape((q_cols, whole), bf16)],
        scratch_shapes=[pltpu.VMEM((block, n1, n2, own, q_cols), bf16)],
        compiler_params=small,
        name="copies",
    )(near_core(units), near_core(rate), near_core(parcels.reshape(n0, n2, n1 * own, parts)))
    copy_v = copy_v.reshape(whole, v_cols)
    return (step_q, step_v, new_q, new_v, first_q, second_q, first_v, second_v, copy_q.T, copy_v)


def solution(mesh):
    split = Mesh(mesh.devices.reshape(12, 8, 2, mesh.shape["tp"]), ("fs_0", "fs_1", "fs_2", "tp"))
    return jax.shard_map(
        on_device,
        mesh=split,
        in_specs=(
            P(FS, None),
            P(FS, "tp"),
            P(FS, "tp"),
            P(FS, None),
            P(FS, None),
            P(FS, "tp"),
            P(FS, "tp"),
            P(FS, "tp"),
            P(FS, "tp"),
            P(FS, "tp"),
            P(FS, "tp"),
        ),
        out_specs=(
            P(FS, "tp"),
            P(FS, "tp"),
            P(FS, "tp"),
            P(FS, "tp"),
            P(FS, "tp"),
            P(FS, "tp"),
            P(FS, "tp"),
            P(FS, "tp"),
            P(None, "tp"),
            P(None, "tp"),
        ),
        check_vma=False,
    )
```

```python
import math

import jax
import jax.numpy as jnp
from jax import lax
from jax.experimental import pallas as pl
from jax.experimental.pallas import tpu as pltpu
from jax.sharding import Mesh
from jax.sharding import PartitionSpec as P

FS = ("fs_0", "fs_1", "fs_2")


first_decay = 0.9
second_decay = 0.99
small_eps = 1e-08
learn_rate = 0.01


def sent_to_all(value, axis):
    size = lax.axis_size(axis)
    return lax.all_to_all(
        jnp.broadcast_to(value[None], (size, *value.shape)), axis, 0, 0, tiled=True
    )


def shift_of(size):
    shift = int(math.log2(size))
    assert 1 << shift == size
    return shift


def pack_kernel(v_factor, q_factor, v_weight, q_weight, spread):
    parcel = jnp.concatenate(
        [
            v_factor[...],
            q_factor[...],
            v_weight[...].astype(jnp.bfloat16),
            q_weight[...].astype(jnp.bfloat16),
        ],
        axis=1,
    )
    spread[...] = jnp.broadcast_to(parcel[None], spread.shape)


def in_lines(share):
    rows, wide = share.shape
    if wide != 96:
        return share
    top = rows * 3 // 4
    extra = [share[top:, 32 * k : 32 * (k + 1)] for k in range(3)]
    return jnp.concatenate([share[:top], jnp.concatenate(extra, axis=0)], axis=1)


def out_of_lines(lines, wide):
    if wide != 96:
        return lines
    part = lines.shape[1] // 3
    extra = [lines[:, part * k : part * (k + 1), 96:] for k in range(3)]
    return jnp.concatenate([lines[:, :, :96], jnp.concatenate(extra, axis=2)], axis=1)


def share_kernel(at, factors, spread, *, sizes, width):
    n0, n1, n2 = sizes
    rank = factors.shape[2] // 2
    row = lax.broadcasted_iota(jnp.int32, (2 * rank, 2 * width), 0)
    col = lax.broadcasted_iota(jnp.int32, (2 * rank, 2 * width), 1)
    of_q = row >= rank
    row = jnp.where(of_q, row - rank, row)
    place = (row & (n1 * n2 - 1)) * n0 + (row >> shift_of(n1 * n2))
    mine = (of_q == (col >= width)) & (
        place == jnp.where(col >= width, col - width, col) + at[0] * width
    )
    mine = mine.astype(jnp.float32).astype(jnp.bfloat16)
    whole = factors[...].reshape(-1, 2 * rank)
    share = jnp.dot(whole, mine, preferred_element_type=jnp.float32)
    spread[...] = jnp.broadcast_to(in_lines(share).astype(jnp.bfloat16)[None], spread.shape)


def project_kernel(lines, inputs, proj, share):
    n0, n1, n2, own, wide = share.shape

    @pl.when(pl.program_id(0) == 0)
    def _():
        for c in range(n2):
            share[:, :, c, :, :] = out_of_lines(lines[c], wide).reshape(n0, n1, own, wide)

    factors = share[...].reshape(-1, wide)
    sums = jnp.dot(inputs[...], factors, preferred_element_type=jnp.float32)
    tokens = inputs.shape[0]
    begin = pl.multiple_of(pl.program_id(0) * tokens, tokens)
    proj[:, pl.ds(begin, tokens)] = sums.astype(jnp.bfloat16).T


def terms_kernel(proj, v_cot, q_cot, blocks, term_v, term_q, wide, *, n0, width):
    rank, v_cols = term_v.shape
    tp = rank // width
    parts = [proj[2 * width * t : 2 * width * (t + 1), :] for t in range(tp)]
    proj_v = jnp.concatenate([p[:width] for p in parts], axis=0)
    proj_q = jnp.concatenate([p[width:] for p in parts], axis=0)
    term_v[...] = jnp.dot(proj_v, v_cot[...], preferred_element_type=jnp.float32)
    term_q[...] = lax.dot_general(
        proj_q, q_cot[...], (((1,), (1,)), ((), ())), preferred_element_type=jnp.float32
    )
    chunks, half = v_cols // 128, n0 // 2
    wide[...] = jnp.zeros(wide.shape, jnp.float32)
    for b in range(rank // n0):
        for k in range(chunks):
            wide[b, n0 * k : n0 * (k + 1), :] = term_v[
                n0 * b : n0 * (b + 1), 128 * k : 128 * (k + 1)
            ]
        wide[b, n0 * chunks : n0 * (chunks + 1), :] = term_q[n0 * b : n0 * (b + 1), :128]
        rest = jnp.concatenate(
            [term_q[n0 * b : n0 * b + half, 128:], term_q[n0 * b + half : n0 * (b + 1), 128:]],
            axis=1,
        )
        wide[b, n0 * (chunks + 1) : n0 * (chunks + 1) + half, :] = rest
    blocks[...] = wide[...].astype(jnp.bfloat16)


def fold_kernel(blocks, rows, wide, *, n0, chunks):
    wide[...] = jnp.sum(blocks[...].astype(jnp.float32), axis=0)
    half = n0 // 2
    rows[...] = jnp.zeros(rows.shape, jnp.float32)
    for r in range(n0):
        for k in range(chunks + 1):
            rows[r, k : k + 1, :] = wide[n0 * k + r : n0 * k + r + 1, :]
        line = n0 * (chunks + 1) + r % half
        rest = wide[line : line + 1, :]
        if r >= half:
            rest = jnp.concatenate([rest[:, 64:], rest[:, :64]], axis=1)
        rows[r, chunks + 1 : chunks + 2, :] = rest


def pieces_of(value):
    high = value.astype(jnp.bfloat16).astype(jnp.float32)
    middle = (value - high).astype(jnp.bfloat16).astype(jnp.float32)
    return high, middle, value - high - middle


def with_pieces(value, block, at):
    lane = lax.broadcasted_iota(jnp.int32, block.shape, 1)
    for k, piece in enumerate(pieces_of(value)):
        block = jnp.where(lane == at + k, piece, block)
    return block


def moments(old_first, old_second, gradient):
    first = first_decay * old_first + (1.0 - first_decay) * gradient
    second = second_decay * old_second + (1.0 - second_decay) * gradient * gradient
    unit = first / (jnp.sqrt(second) + small_eps)
    return (first, second, unit)


def moments_kernel(terms, v_first, v_second, q_first, q_second, *outs):
    first_v, second_v, first_q, second_q, spread = outs
    v_cols, q_cols = v_first.shape[1], q_first.shape[1]
    gradient = jnp.sum(terms[...], axis=0)
    gradient = jnp.concatenate(
        [gradient[k : k + 1] for k in range(v_cols // 128 + 1)]
        + [gradient[v_cols // 128 + 1 : v_cols // 128 + 2, : q_cols - 128]],
        axis=1,
    )
    first_v[...], second_v[...], unit_v = moments(v_first[...], v_second[...], gradient[:, :v_cols])
    first_q[...], second_q[...], unit_q = moments(q_first[...], q_second[...], gradient[:, v_cols:])
    squares = jnp.sum(unit_v * unit_v, axis=1, keepdims=True)
    squares += jnp.sum(unit_q * unit_q, axis=1, keepdims=True)
    cols = gradient.shape[1]
    lines = -(-(cols + 3) // 128)
    row = jnp.concatenate(
        [unit_v, unit_q, jnp.zeros((1, lines * 128 - cols), jnp.float32)], axis=1
    )
    row = with_pieces(squares, row, cols)
    block = jnp.concatenate(
        [row[:, 128 * k : 128 * (k + 1)] for k in range(lines)]
        + [jnp.zeros((spread.shape[1] - lines, 128), jnp.float32)],
        axis=0,
    ).astype(jnp.bfloat16)
    spread[...] = jnp.broadcast_to(block[None], spread.shape)


def regroup_kernel(at, blocks, spread, *, cols):
    n1, tp = blocks.shape[:2]
    lines = spread.shape[2] // 128
    last, begin = cols // 128, cols % 128
    ends = blocks[:, :, last, :].astype(jnp.float32)
    ends = jnp.sum(ends, axis=1)
    lane = lax.broadcasted_iota(jnp.int32, ends.shape, 1)
    squares = jnp.where((lane >= begin) & (lane < begin + 3), ends, 0.0)
    squares = jnp.sum(squares, axis=1, keepdims=True)
    own = blocks[:, at[0], :, :].astype(jnp.float32)
    parts = [own[:, k, :] for k in range(lines)]
    parts[last] = with_pieces(squares, parts[last], begin)
    rows = jnp.concatenate(parts, axis=1).astype(jnp.bfloat16)
    spread[...] = jnp.broadcast_to(rows[None], spread.shape)


def finish_kernel(
    rows, v_factor, q_factor, v_weight, q_weight, step_v, step_q, new_v, new_q, units, rate,
    *, sizes, v_cols, entries
):
    rank = rows.shape[0]
    cols = units.shape[1]
    n0, n1, n2 = sizes
    tail = rows[:, cols // 128 * 128 :].astype(jnp.float32)
    lane = lax.broadcasted_iota(jnp.int32, tail.shape, 1) + cols // 128 * 128
    total = jnp.sum(jnp.where((lane >= cols) & (lane < cols + 3), tail, 0.0), keepdims=True)
    scale = lax.rsqrt(total / entries + 1e-06)
    rate[...] = jnp.broadcast_to(learn_rate * scale, rate.shape)
    row = lax.broadcasted_iota(jnp.int32, (rank, rank), 0)
    far = row >> shift_of(n1 * n2)
    place = (row & (n2 - 1)) * (n0 * n1) + far * n1 + ((row >> shift_of(n2)) & (n1 - 1))
    turn = place == lax.broadcasted_iota(jnp.int32, (rank, rank), 1)
    turn = turn.astype(jnp.float32).astype(jnp.bfloat16)
    turned = jnp.dot(turn, rows[...], preferred_element_type=jnp.float32).astype(jnp.bfloat16)
    units[:rank, :v_cols] = turned[:, :v_cols]
    units[rank:, :v_cols] = jnp.zeros((rank, v_cols), units.dtype)
    units[:rank, v_cols:] = jnp.zeros((rank, cols - v_cols), units.dtype)
    units[rank:, v_cols:] = turned[:, v_cols:cols]
    step = scale * jnp.dot(v_factor[...], turned[:, :v_cols], preferred_element_type=jnp.float32)
    step_v[...] = step
    new_v[...] = v_weight[...] - learn_rate * step
    step = scale * jnp.dot(
        q_factor[...], turned[:, v_cols:cols], preferred_element_type=jnp.float32
    )
    step_q[...] = step
    new_q[...] = q_weight[...] - learn_rate * step


def copies_kernel(units, rate, parcels, copy_v, copy_q, turned, *, rank, v_cols):
    to_v, from_q = min(rank + -rank % 128, 2 * rank), rank // 128 * 128
    block, n1, n2, own, q_cols = turned.shape
    part = parcels[pl.ds(pl.program_id(0) * block, block)].reshape(-1, parcels.shape[-1])
    weights = part[:, 2 * rank :].astype(jnp.float32)
    step = jnp.dot(part[:, :to_v], units[:to_v, :v_cols], preferred_element_type=jnp.float32)
    new = (weights[:, :v_cols] - rate[:, :v_cols] * step).astype(jnp.bfloat16)
    new = new.reshape(block, n2, n1, own, v_cols)
    for c in range(n2):
        copy_v[:, :, c, :, :] = new[:, c]
    step = jnp.dot(
        part[:, from_q : 2 * rank], units[from_q:, v_cols:], preferred_element_type=jnp.float32
    )
    new = (weights[:, v_cols:] - rate[:, v_cols:] * step).astype(jnp.bfloat16)
    new = new.reshape(block, n2, n1, own, q_cols)
    for c in range(n2):
        turned[:, :, c, :, :] = new[:, c]
    copy_q[...] = turned[...].reshape(-1, q_cols).T


def on_device(
    inputs,
    query_cot,
    value_cot,
    query_factor,
    value_factor,
    query_weight,
    value_weight,
    query_first,
    query_second,
    value_first,
    value_second,
):
    sizes = tuple(lax.axis_size(a) for a in FS)
    n0, n1, n2 = sizes
    tp = lax.axis_size("tp")
    own, rank = query_factor.shape
    q_cols = query_cot.shape[1]
    v_cols = value_cot.shape[1]
    cols = q_cols + v_cols
    width = rank // tp
    whole = rank * own
    bf16, f32 = jnp.bfloat16, jnp.float32
    shape = jax.ShapeDtypeStruct
    vmem = pl.BlockSpec(memory_space=pltpu.VMEM)
    smem = pl.BlockSpec(memory_space=pltpu.SMEM)
    small = pltpu.CompilerParams(vmem_limit_bytes=16 * 1024 * 1024)
    waits = pl.CostEstimate(flops=20_000_000_000, transcendentals=0, bytes_accessed=1_000_000)
    near_core = lambda a: pltpu.with_memory_space_constraint(a, pltpu.VMEM)
    at = lax.axis_index("tp").astype(jnp.int32).reshape(1)

    parts = 2 * rank + cols
    spread = pl.pallas_call(
        pack_kernel,
        in_specs=[vmem] * 4,
        out_specs=vmem,
        out_shape=pltpu.VMEM((n1, own, parts), bf16),
        name="pack",
    )(value_factor, query_factor, value_weight, query_weight)
    near = lax.all_to_all(spread, "fs_1", 0, 0, tiled=True)
    parcel = near.reshape(n1 * own, parts)

    lines = (n1 * own * 3 // 4, 128) if 2 * width == 96 else (n1 * own, 2 * width)
    spread = pl.pallas_call(
        lambda *refs: share_kernel(*refs, sizes=sizes, width=width),
        grid=(1,),
        in_specs=[smem, pl.BlockSpec((n1, own, 2 * rank), lambda i: (0, 0, 0))],
        out_specs=vmem,
        out_shape=pltpu.VMEM((n0, *lines), bf16),
        compiler_params=small,
        cost_estimate=waits,
        name="share",
    )(at, near)
    near = lax.all_to_all(spread, "fs_0", 0, 0, tiled=True)
    near, parcel = lax.optimization_barrier((near, parcel))
    parcels = lax.all_gather(parcel, ("fs_0", "fs_2"), axis=0, tiled=True)
    near = sent_to_all(near, "fs_2").reshape(n2, n0, *lines)
    proj = pl.pallas_call(
        project_kernel,
        grid=(4,),
        in_specs=[vmem, pl.BlockSpec((inputs.shape[0] // 4, inputs.shape[1]), lambda i: (i, 0))],
        out_specs=vmem,
        out_shape=pltpu.VMEM((2 * width, inputs.shape[0]), bf16),
        scratch_shapes=[pltpu.VMEM((n0, n1, n2, own, 2 * width), bf16)],
        name="project",
    )(near_core(near), inputs)
    proj = lax.all_gather(proj, "tp", axis=0, tiled=True)

    chunks = v_cols // 128
    lines = n0 * (chunks + 1) + n0 // 2
    lines += -lines % 8
    blocks = pl.pallas_call(
        lambda *refs: terms_kernel(*refs, n0=n0, width=width),
        in_specs=[vmem] * 3,
        out_specs=vmem,
        out_shape=pltpu.VMEM((n1 * n2, lines, 128), bf16),
        scratch_shapes=[
            pltpu.VMEM((rank, v_cols), f32),
            pltpu.VMEM((rank, q_cols), f32),
            pltpu.VMEM((n1 * n2, lines, 128), f32),
        ],
        name="terms",
    )(near_core(proj), near_core(value_cot), near_core(query_cot.T))
    blocks = lax.all_to_all(blocks, ("fs_1", "fs_2"), 0, 0, tiled=True)
    term = pl.pallas_call(
        lambda *refs: fold_kernel(*refs, n0=n0, chunks=chunks),
        in_specs=[vmem],
        out_specs=vmem,
        out_shape=pltpu.VMEM((n0, 8, 128), f32),
        scratch_shapes=[pltpu.VMEM((lines, 128), f32)],
        name="fold",
    )(near_core(blocks))
    term = lax.all_to_all(term, "fs_0", 0, 0, tiled=True)
    first_v, second_v, first_q, second_q, spread = pl.pallas_call(
        moments_kernel,
        in_specs=[vmem] * 5,
        out_specs=[vmem] * 5,
        out_shape=[shape((1, v_cols), f32)] * 2
        + [shape((1, q_cols), f32)] * 2
        + [pltpu.VMEM((n1 * tp, 8, 128), bf16)],
        name="moments",
    )(
        near_core(term),
        near_core(value_first),
        near_core(value_second),
        near_core(query_first),
        near_core(query_second),
    )

    blocks = lax.all_to_all(spread, ("fs_1", "tp"), 0, 0, tiled=True)
    lines = -(-(cols + 3) // 128)
    spread = pl.pallas_call(
        lambda *refs: regroup_kernel(*refs, cols=cols),
        in_specs=[smem, vmem],
        out_specs=vmem,
        out_shape=pltpu.VMEM((n0, n1, lines * 128), bf16),
        compiler_params=small,
        cost_estimate=waits,
        name="regroup",
    )(at, near_core(blocks.reshape(n1, tp, 8, 128)))
    rows = lax.all_to_all(spread, "fs_0", 0, 0, tiled=True).reshape(n0 * n1, -1)
    rows, parcels = lax.optimization_barrier((rows, parcels))
    rows = sent_to_all(rows, "fs_2").reshape(rank, -1)

    step_v, step_q, new_v, new_q, units, rate = pl.pallas_call(
        lambda *refs: finish_kernel(*refs, sizes=sizes, v_cols=v_cols, entries=rank * cols * tp),
        in_specs=[vmem] * 5,
        out_specs=[vmem] * 6,
        out_shape=[
            shape((own, v_cols), f32),
            shape((own, q_cols), f32),
            shape((own, v_cols), f32),
            shape((own, q_cols), f32),
            pltpu.VMEM((2 * rank, cols), bf16),
            pltpu.VMEM((1, cols), f32),
        ],
        compiler_params=small,
        cost_estimate=waits,
        name="finish",
    )(
        near_core(rows),
        near_core(value_factor),
        near_core(query_factor),
        near_core(value_weight),
        near_core(query_weight),
    )

    steps = 4
    block = n0 // steps
    copy_v, copy_q = pl.pallas_call(
        lambda *refs: copies_kernel(*refs, rank=rank, v_cols=v_cols),
        grid=(steps,),
        in_specs=[
            vmem,
            vmem,
            vmem,
        ],
        out_specs=[
            pl.BlockSpec((block, n1, n2, own, v_cols), lambda i: (i, 0, 0, 0, 0)),
            pl.BlockSpec((q_cols, whole // steps), lambda i: (0, i)),
        ],
        out_shape=[shape((n0, n1, n2, own, v_cols), bf16), shape((q_cols, whole), bf16)],
        scratch_shapes=[pltpu.VMEM((block, n1, n2, own, q_cols), bf16)],
        compiler_params=small,
        name="copies",
    )(near_core(units), near_core(rate), near_core(parcels.reshape(n0, n2, n1 * own, parts)))
    copy_v = copy_v.reshape(whole, v_cols)
    return (step_q, step_v, new_q, new_v, first_q, second_q, first_v, second_v, copy_q.T, copy_v)


def solution(mesh):
    split = Mesh(mesh.devices.reshape(12, 8, 2, mesh.shape["tp"]), ("fs_0", "fs_1", "fs_2", "tp"))
    return jax.shard_map(
        on_device,
        mesh=split,
        in_specs=(
            P(FS, None),
            P(FS, "tp"),
            P(FS, "tp"),
            P(FS, None),
            P(FS, None),
            P(FS, "tp"),
            P(FS, "tp"),
            P(FS, "tp"),
            P(FS, "tp"),
            P(FS, "tp"),
            P(FS, "tp"),
        ),
        out_specs=(
            P(FS, "tp"),
            P(FS, "tp"),
            P(FS, "tp"),
            P(FS, "tp"),
            P(FS, "tp"),
            P(FS, "tp"),
            P(FS, "tp"),
            P(FS, "tp"),
            P(None, "tp"),
            P(None, "tp"),
        ),
        check_vma=False,
    )
```

```python
import math

import jax
import jax.numpy as jnp
from jax import lax
from jax.experimental import pallas as pl
from jax.experimental.pallas import tpu as pltpu
from jax.sharding import Mesh
from jax.sharding import PartitionSpec as P

FS = ("fs_0", "fs_1", "fs_2")


first_decay = 0.9
second_decay = 0.99
small_eps = 1e-08
learn_rate = 0.01


def sent_to_all(value, axis):
    size = lax.axis_size(axis)
    return lax.all_to_all(
        jnp.broadcast_to(value[None], (size, *value.shape)), axis, 0, 0, tiled=True
    )


def shift_of(size):
    shift = int(math.log2(size))
    assert 1 << shift == size
    return shift


def pack_kernel(v_factor, q_factor, v_weight, q_weight, spread):
    parcel = jnp.concatenate(
        [
            v_factor[...],
            q_factor[...],
            v_weight[...].astype(jnp.bfloat16),
            q_weight[...].astype(jnp.bfloat16),
        ],
        axis=1,
    )
    spread[...] = jnp.broadcast_to(parcel[None], spread.shape)


def in_lines(share):
    rows, wide = share.shape
    if wide != 96:
        return share
    top = rows * 3 // 4
    extra = [share[top:, 32 * k : 32 * (k + 1)] for k in range(3)]
    return jnp.concatenate([share[:top], jnp.concatenate(extra, axis=0)], axis=1)


def out_of_lines(lines, wide):
    if wide != 96:
        return lines
    part = lines.shape[1] // 3
    extra = [lines[:, part * k : part * (k + 1), 96:] for k in range(3)]
    return jnp.concatenate([lines[:, :, :96], jnp.concatenate(extra, axis=2)], axis=1)


def share_kernel(at, factors, spread, *, sizes, width):
    n0, n1, n2 = sizes
    rank = factors.shape[2] // 2
    row = lax.broadcasted_iota(jnp.int32, (2 * rank, 2 * width), 0)
    col = lax.broadcasted_iota(jnp.int32, (2 * rank, 2 * width), 1)
    of_q = row >= rank
    row = jnp.where(of_q, row - rank, row)
    place = (row & (n1 * n2 - 1)) * n0 + (row >> shift_of(n1 * n2))
    mine = (of_q == (col >= width)) & (
        place == jnp.where(col >= width, col - width, col) + at[0] * width
    )
    mine = mine.astype(jnp.float32).astype(jnp.bfloat16)
    whole = factors[...].reshape(-1, 2 * rank)
    share = jnp.dot(whole, mine, preferred_element_type=jnp.float32)
    spread[...] = jnp.broadcast_to(in_lines(share).astype(jnp.bfloat16)[None], spread.shape)


def project_kernel(lines, inputs, proj, share):
    n0, n1, n2, own, wide = share.shape
    for c in range(n2):
        share[:, :, c, :, :] = out_of_lines(lines[c], wide).reshape(n0, n1, own, wide)
    factors = share[...].reshape(-1, wide)
    sums = jnp.dot(inputs[...], factors, preferred_element_type=jnp.float32)
    proj[...] = sums.astype(jnp.bfloat16).T


def terms_kernel(proj, v_cot, q_cot, blocks, term_v, term_q, wide, *, n0, width):
    rank, v_cols = term_v.shape
    tp = rank // width
    parts = [proj[2 * width * t : 2 * width * (t + 1), :] for t in range(tp)]
    proj_v = jnp.concatenate([p[:width] for p in parts], axis=0)
    proj_q = jnp.concatenate([p[width:] for p in parts], axis=0)
    term_v[...] = jnp.dot(proj_v, v_cot[...], preferred_element_type=jnp.float32)
    term_q[...] = lax.dot_general(
        proj_q, q_cot[...], (((1,), (1,)), ((), ())), preferred_element_type=jnp.float32
    )
    chunks, half = v_cols // 128, n0 // 2
    wide[...] = jnp.zeros(wide.shape, jnp.float32)
    for b in range(rank // n0):
        for k in range(chunks):
            wide[b, n0 * k : n0 * (k + 1), :] = term_v[
                n0 * b : n0 * (b + 1), 128 * k : 128 * (k + 1)
            ]
        wide[b, n0 * chunks : n0 * (chunks + 1), :] = term_q[n0 * b : n0 * (b + 1), :128]
        rest = jnp.concatenate(
            [term_q[n0 * b : n0 * b + half, 128:], term_q[n0 * b + half : n0 * (b + 1), 128:]],
            axis=1,
        )
        wide[b, n0 * (chunks + 1) : n0 * (chunks + 1) + half, :] = rest
    blocks[...] = wide[...].astype(jnp.bfloat16)


def fold_kernel(blocks, rows, wide, *, n0, chunks):
    wide[...] = jnp.sum(blocks[...].astype(jnp.float32), axis=0)
    half = n0 // 2
    rows[...] = jnp.zeros(rows.shape, jnp.float32)
    for r in range(n0):
        for k in range(chunks + 1):
            rows[r, k : k + 1, :] = wide[n0 * k + r : n0 * k + r + 1, :]
        line = n0 * (chunks + 1) + r % half
        rest = wide[line : line + 1, :]
        if r >= half:
            rest = jnp.concatenate([rest[:, 64:], rest[:, :64]], axis=1)
        rows[r, chunks + 1 : chunks + 2, :] = rest


def pieces_of(value):
    high = value.astype(jnp.bfloat16).astype(jnp.float32)
    middle = (value - high).astype(jnp.bfloat16).astype(jnp.float32)
    return high, middle, value - high - middle


def with_pieces(value, block, at):
    lane = lax.broadcasted_iota(jnp.int32, block.shape, 1)
    for k, piece in enumerate(pieces_of(value)):
        block = jnp.where(lane == at + k, piece, block)
    return block


def moments(old_first, old_second, gradient):
    first = first_decay * old_first + (1.0 - first_decay) * gradient
    second = second_decay * old_second + (1.0 - second_decay) * gradient * gradient
    unit = first / (jnp.sqrt(second) + small_eps)
    return (first, second, unit)


def moments_kernel(terms, v_first, v_second, q_first, q_second, *outs):
    first_v, second_v, first_q, second_q, spread = outs
    v_cols, q_cols = v_first.shape[1], q_first.shape[1]
    gradient = jnp.sum(terms[...], axis=0)
    gradient = jnp.concatenate(
        [gradient[k : k + 1] for k in range(v_cols // 128 + 1)]
        + [gradient[v_cols // 128 + 1 : v_cols // 128 + 2, : q_cols - 128]],
        axis=1,
    )
    first_v[...], second_v[...], unit_v = moments(v_first[...], v_second[...], gradient[:, :v_cols])
    first_q[...], second_q[...], unit_q = moments(q_first[...], q_second[...], gradient[:, v_cols:])
    squares = jnp.sum(unit_v * unit_v, axis=1, keepdims=True)
    squares += jnp.sum(unit_q * unit_q, axis=1, keepdims=True)
    cols = gradient.shape[1]
    lines = -(-(cols + 3) // 128)
    row = jnp.concatenate(
        [unit_v, unit_q, jnp.zeros((1, lines * 128 - cols), jnp.float32)], axis=1
    )
    row = with_pieces(squares, row, cols)
    block = jnp.concatenate(
        [row[:, 128 * k : 128 * (k + 1)] for k in range(lines)]
        + [jnp.zeros((spread.shape[1] - lines, 128), jnp.float32)],
        axis=0,
    ).astype(jnp.bfloat16)
    spread[...] = jnp.broadcast_to(block[None], spread.shape)


def regroup_kernel(at, blocks, spread, *, cols):
    n1, tp = blocks.shape[:2]
    lines = spread.shape[2] // 128
    last, begin = cols // 128, cols % 128
    ends = blocks[:, :, last, :].astype(jnp.float32)
    ends = jnp.sum(ends, axis=1)
    lane = lax.broadcasted_iota(jnp.int32, ends.shape, 1)
    squares = jnp.where((lane >= begin) & (lane < begin + 3), ends, 0.0)
    squares = jnp.sum(squares, axis=1, keepdims=True)
    own = blocks[:, at[0], :, :].astype(jnp.float32)
    parts = [own[:, k, :] for k in range(lines)]
    parts[last] = with_pieces(squares, parts[last], begin)
    rows = jnp.concatenate(parts, axis=1).astype(jnp.bfloat16)
    spread[...] = jnp.broadcast_to(rows[None], spread.shape)


def finish_kernel(
    rows, v_factor, q_factor, v_weight, q_weight, step_v, step_q, new_v, new_q, units, rate,
    *, sizes, v_cols, entries
):
    rank = rows.shape[0]
    cols = units.shape[1]
    n0, n1, n2 = sizes
    tail = rows[:, cols // 128 * 128 :].astype(jnp.float32)
    lane = lax.broadcasted_iota(jnp.int32, tail.shape, 1) + cols // 128 * 128
    total = jnp.sum(jnp.where((lane >= cols) & (lane < cols + 3), tail, 0.0), keepdims=True)
    scale = lax.rsqrt(total / entries + 1e-06)
    rate[...] = jnp.broadcast_to(learn_rate * scale, rate.shape)
    row = lax.broadcasted_iota(jnp.int32, (rank, rank), 0)
    far = row >> shift_of(n1 * n2)
    place = (row & (n2 - 1)) * (n0 * n1) + far * n1 + ((row >> shift_of(n2)) & (n1 - 1))
    turn = place == lax.broadcasted_iota(jnp.int32, (rank, rank), 1)
    turn = turn.astype(jnp.float32).astype(jnp.bfloat16)
    turned = jnp.dot(turn, rows[...], preferred_element_type=jnp.float32).astype(jnp.bfloat16)
    units[:rank, :v_cols] = turned[:, :v_cols]
    units[rank:, :v_cols] = jnp.zeros((rank, v_cols), units.dtype)
    units[:rank, v_cols:] = jnp.zeros((rank, cols - v_cols), units.dtype)
    units[rank:, v_cols:] = turned[:, v_cols:cols]
    step = scale * jnp.dot(v_factor[...], turned[:, :v_cols], preferred_element_type=jnp.float32)
    step_v[...] = step
    new_v[...] = v_weight[...] - learn_rate * step
    step = scale * jnp.dot(
        q_factor[...], turned[:, v_cols:cols], preferred_element_type=jnp.float32
    )
    step_q[...] = step
    new_q[...] = q_weight[...] - learn_rate * step


def copies_kernel(units, rate, parcels, copy_v, copy_q, turned, *, rank, v_cols):
    to_v, from_q = min(rank + -rank % 128, 2 * rank), rank // 128 * 128
    block, n1, n2, own, q_cols = turned.shape
    part = parcels[pl.ds(pl.program_id(0) * block, block)].reshape(-1, parcels.shape[-1])
    weights = part[:, 2 * rank :].astype(jnp.float32)
    step = jnp.dot(part[:, :to_v], units[:to_v, :v_cols], preferred_element_type=jnp.float32)
    new = (weights[:, :v_cols] - rate[:, :v_cols] * step).astype(jnp.bfloat16)
    new = new.reshape(block, n2, n1, own, v_cols)
    for c in range(n2):
        copy_v[:, :, c, :, :] = new[:, c]
    step = jnp.dot(
        part[:, from_q : 2 * rank], units[from_q:, v_cols:], preferred_element_type=jnp.float32
    )
    new = (weights[:, v_cols:] - rate[:, v_cols:] * step).astype(jnp.bfloat16)
    new = new.reshape(block, n2, n1, own, q_cols)
    for c in range(n2):
        turned[:, :, c, :, :] = new[:, c]
    copy_q[...] = turned[...].reshape(-1, q_cols).T


def on_device(
    inputs,
    query_cot,
    value_cot,
    query_factor,
    value_factor,
    query_weight,
    value_weight,
    query_first,
    query_second,
    value_first,
    value_second,
):
    sizes = tuple(lax.axis_size(a) for a in FS)
    n0, n1, n2 = sizes
    tp = lax.axis_size("tp")
    own, rank = query_factor.shape
    q_cols = query_cot.shape[1]
    v_cols = value_cot.shape[1]
    cols = q_cols + v_cols
    width = rank // tp
    whole = rank * own
    bf16, f32 = jnp.bfloat16, jnp.float32
    shape = jax.ShapeDtypeStruct
    vmem = pl.BlockSpec(memory_space=pltpu.VMEM)
    smem = pl.BlockSpec(memory_space=pltpu.SMEM)
    small = pltpu.CompilerParams(vmem_limit_bytes=16 * 1024 * 1024)
    waits = pl.CostEstimate(flops=20_000_000_000, transcendentals=0, bytes_accessed=1_000_000)
    near_core = lambda a: pltpu.with_memory_space_constraint(a, pltpu.VMEM)
    at = lax.axis_index("tp").astype(jnp.int32).reshape(1)

    parts = 2 * rank + cols
    spread = pl.pallas_call(
        pack_kernel,
        in_specs=[vmem] * 4,
        out_specs=vmem,
        out_shape=pltpu.VMEM((n1, own, parts), bf16),
        name="pack",
    )(value_factor, query_factor, value_weight, query_weight)
    near = lax.all_to_all(spread, "fs_1", 0, 0, tiled=True)
    parcels = lax.all_gather(near.reshape(n1 * own, parts), ("fs_0", "fs_2"), axis=0, tiled=True)

    lines = (n1 * own * 3 // 4, 128) if 2 * width == 96 else (n1 * own, 2 * width)
    spread = pl.pallas_call(
        lambda *refs: share_kernel(*refs, sizes=sizes, width=width),
        grid=(1,),
        in_specs=[smem, pl.BlockSpec((n1, own, 2 * rank), lambda i: (0, 0, 0))],
        out_specs=vmem,
        out_shape=pltpu.VMEM((n0, *lines), bf16),
        compiler_params=small,
        cost_estimate=waits,
        name="share",
    )(at, pltpu.with_memory_space_constraint(near, pltpu.HBM))
    near = lax.all_to_all(spread, "fs_0", 0, 0, tiled=True)
    near = sent_to_all(near, "fs_2").reshape(n2, n0, *lines)
    proj = pl.pallas_call(
        project_kernel,
        in_specs=[vmem] * 2,
        out_specs=vmem,
        out_shape=pltpu.VMEM((2 * width, inputs.shape[0]), bf16),
        scratch_shapes=[pltpu.VMEM((n0, n1, n2, own, 2 * width), bf16)],
        compiler_params=small,
        name="project",
    )(near_core(near), near_core(inputs))
    proj = lax.all_gather(proj, "tp", axis=0, tiled=True)

    chunks = v_cols // 128
    lines = n0 * (chunks + 1) + n0 // 2
    lines += -lines % 8
    blocks = pl.pallas_call(
        lambda *refs: terms_kernel(*refs, n0=n0, width=width),
        in_specs=[vmem] * 3,
        out_specs=vmem,
        out_shape=pltpu.VMEM((n1 * n2, lines, 128), bf16),
        scratch_shapes=[
            pltpu.VMEM((rank, v_cols), f32),
            pltpu.VMEM((rank, q_cols), f32),
            pltpu.VMEM((n1 * n2, lines, 128), f32),
        ],
        name="terms",
    )(near_core(proj), near_core(value_cot), near_core(query_cot.T))
    blocks = lax.all_to_all(blocks, ("fs_1", "fs_2"), 0, 0, tiled=True)
    term = pl.pallas_call(
        lambda *refs: fold_kernel(*refs, n0=n0, chunks=chunks),
        in_specs=[vmem],
        out_specs=vmem,
        out_shape=pltpu.VMEM((n0, 8, 128), f32),
        scratch_shapes=[pltpu.VMEM((lines, 128), f32)],
        name="fold",
    )(near_core(blocks))
    term = lax.all_to_all(term, "fs_0", 0, 0, tiled=True)
    first_v, second_v, first_q, second_q, spread = pl.pallas_call(
        moments_kernel,
        in_specs=[vmem] * 5,
        out_specs=[vmem] * 5,
        out_shape=[shape((1, v_cols), f32)] * 2
        + [shape((1, q_cols), f32)] * 2
        + [pltpu.VMEM((n1 * tp, 8, 128), bf16)],
        name="moments",
    )(
        near_core(term),
        near_core(value_first),
        near_core(value_second),
        near_core(query_first),
        near_core(query_second),
    )

    spread, parcels = lax.optimization_barrier((spread, parcels))
    blocks = lax.all_to_all(spread, ("fs_1", "tp"), 0, 0, tiled=True)
    lines = -(-(cols + 3) // 128)
    spread = pl.pallas_call(
        lambda *refs: regroup_kernel(*refs, cols=cols),
        in_specs=[smem, vmem],
        out_specs=vmem,
        out_shape=pltpu.VMEM((n0, n1, lines * 128), bf16),
        compiler_params=small,
        cost_estimate=waits,
        name="regroup",
    )(at, near_core(blocks.reshape(n1, tp, 8, 128)))
    rows = lax.all_to_all(spread, "fs_0", 0, 0, tiled=True).reshape(n0 * n1, -1)
    rows = sent_to_all(rows, "fs_2").reshape(rank, -1)

    step_v, step_q, new_v, new_q, units, rate = pl.pallas_call(
        lambda *refs: finish_kernel(*refs, sizes=sizes, v_cols=v_cols, entries=rank * cols * tp),
        in_specs=[vmem] * 5,
        out_specs=[vmem] * 6,
        out_shape=[
            shape((own, v_cols), f32),
            shape((own, q_cols), f32),
            shape((own, v_cols), f32),
            shape((own, q_cols), f32),
            pltpu.VMEM((2 * rank, cols), bf16),
            pltpu.VMEM((1, cols), f32),
        ],
        compiler_params=small,
        cost_estimate=waits,
        name="finish",
    )(
        near_core(rows),
        near_core(value_factor),
        near_core(query_factor),
        near_core(value_weight),
        near_core(query_weight),
    )

    steps = 2
    block = n0 // steps
    copy_v, copy_q = pl.pallas_call(
        lambda *refs: copies_kernel(*refs, rank=rank, v_cols=v_cols),
        grid=(steps,),
        in_specs=[
            vmem,
            vmem,
            vmem,
        ],
        out_specs=[
            pl.BlockSpec((block, n1, n2, own, v_cols), lambda i: (i, 0, 0, 0, 0)),
            pl.BlockSpec((q_cols, whole // steps), lambda i: (0, i)),
        ],
        out_shape=[shape((n0, n1, n2, own, v_cols), bf16), shape((q_cols, whole), bf16)],
        scratch_shapes=[pltpu.VMEM((block, n1, n2, own, q_cols), bf16)],
        compiler_params=small,
        name="copies",
    )(near_core(units), near_core(rate), near_core(parcels.reshape(n0, n2, n1 * own, parts)))
    copy_v = copy_v.reshape(whole, v_cols)
    return (step_q, step_v, new_q, new_v, first_q, second_q, first_v, second_v, copy_q.T, copy_v)


def solution(mesh):
    split = Mesh(mesh.devices.reshape(12, 8, 2, mesh.shape["tp"]), ("fs_0", "fs_1", "fs_2", "tp"))
    return jax.shard_map(
        on_device,
        mesh=split,
        in_specs=(
            P(FS, None),
            P(FS, "tp"),
            P(FS, "tp"),
            P(FS, None),
            P(FS, None),
            P(FS, "tp"),
            P(FS, "tp"),
            P(FS, "tp"),
            P(FS, "tp"),
            P(FS, "tp"),
            P(FS, "tp"),
        ),
        out_specs=(
            P(FS, "tp"),
            P(FS, "tp"),
            P(FS, "tp"),
            P(FS, "tp"),
            P(FS, "tp"),
            P(FS, "tp"),
            P(FS, "tp"),
            P(FS, "tp"),
            P(None, "tp"),
            P(None, "tp"),
        ),
        check_vma=False,
    )
```
